512 devices in a mesh: kv: 64 (over z, y), tp: 8 (over x, core).
Axes of the slice: x: 4, y: 4, z: 16, core: 2. Of those that a mesh axis runs over, the one named last changes fastest.
Arguments:
- stream: bfloat16 [32, 4096], P(None, 'kv'), may hold values from -32 to 32
- gain_in: bfloat16 [4096], P('kv'), may hold values from 0.099609375 to 1.8984375
- w_query: bfloat16 [4096, 2048], P('kv', 'tp'), may hold values from -0.09375 to 0.09375
- w_key: bfloat16 [4096, 2048], P('kv', 'tp'), may hold values from -0.09375 to 0.09375
- w_value: bfloat16 [4096, 2048], P('kv', 'tp'), may hold values from -0.09375 to 0.09375
- w_forget: bfloat16 [4096, 16], replicated, may hold values from -0.09375 to 0.09375
- keys_cache: bfloat16 [32, 16, 8192, 128], P(None, 'tp', 'kv'), may hold values from -136 to 136
- values_cache: bfloat16 [32, 16, 8192, 128], P(None, 'tp', 'kv'), may hold values from -6 to 6
- decay_cache: float32 [32, 16, 8192], P(None, 'tp', 'kv'), may hold values from -1283 to 0
- lengths: int32 [32], replicated, may hold values from 1 to 8192, 104889 in all
- gain_att: bfloat16 [2048], P('tp'), may hold values from 0.099609375 to 1.8984375
- w_out: bfloat16 [2048, 4096], P('tp', 'kv'), may hold values from -0.125 to 0.125
- gain_mlp: bfloat16 [4096], P('kv'), may hold values from 0.099609375 to 1.8984375
- w_up: bfloat16 [4096, 16384], P('kv', 'tp'), may hold values from -0.09375 to 0.09375
- w_down: bfloat16 [16384, 4096], P('tp', 'kv'), may hold values from -0.046875 to 0.046875
Outputs:
- updated: bfloat16 [32, 4096], P(None, 'kv')
The draws below stay inside these ranges and needn't reach their ends.
Inputs may be any that keep to these rules, and one draw needn't show every extreme that they name: `lengths`: one sequence has all 8192 positions live.
All inputs are finite; a program needn't handle non-finite values.
Results may differ from the reference program's by a relative error of at most 0.012.
The reference program's roundings to bfloat16 on the way count: a program that leaves them out, or rounds other values in their place, can miss the bound.
Values may be sent and summed in bfloat16 or wider, within the bound.
No kernel may reach another device: no remote copies, remote signals or barrier semaphores. Data moves between devices by JAX's collectives and lax.ppermute only.
A program may use at most 64 MiB of HBM per device.

```python
import math
import jax
import jax.numpy as jnp
import numpy as np
from jax import lax

D = 4096
HEAD_COUNT = 16
HEAD_WIDTH = 128
FF = 16384
SEQUENCE_COUNT = 32
POS_DEV = 128
CACHE_LENGTH = 8192
HW = 2048


def draw_stream(key, part):
    key_one, key_two = jax.random.split(jax.random.fold_in(key, 11), 2)
    column = jnp.arange(D, dtype=jnp.float32) / D
    raw_values = jnp.clip(jax.random.normal(key_one, (SEQUENCE_COUNT, D), jnp.float32), -5.0, 5.0)
    column_scale = jnp.exp(math.log(10.0) * (column - 0.5))
    row_scale = jnp.exp(jax.random.uniform(key_two, (SEQUENCE_COUNT, 1), jnp.float32, math.log(0.5), math.log(2.0)))
    return (raw_values * column_scale[None, :] * row_scale).astype(jnp.bfloat16)


def draw_keys_cache(key, part):
    key_one = jax.random.fold_in(jax.random.fold_in(key, 5), 0)
    full_shape = (SEQUENCE_COUNT, HEAD_COUNT, CACHE_LENGTH, HEAD_WIDTH)
    raw_values = jnp.clip(jax.random.normal(key_one, full_shape, jnp.float32), -5.0, 5.0)
    return raw_values.astype(jnp.bfloat16)


def draw_decay_cache(key, part):
    every_key = jax.random.split(jax.random.fold_in(key, 23), 7)
    head_order = jax.random.permutation(every_key[0], HEAD_COUNT)
    keep_count = HEAD_COUNT // 2
    slow_heads = (head_order < keep_count).reshape(1, HEAD_COUNT, 1)
    slow_rate = jax.random.uniform(every_key[1], (SEQUENCE_COUNT, HEAD_COUNT, 1), jnp.float32, 0.2, 0.8) / CACHE_LENGTH
    fast_rate = 1.0 / (POS_DEV * jax.random.uniform(every_key[2], (SEQUENCE_COUNT, HEAD_COUNT, 1), jnp.float32, 0.25, 0.8))
    learning_rate = jnp.where(slow_heads, slow_rate, fast_rate)
    jaggedness = jnp.exp(jax.random.uniform(every_key[3], (SEQUENCE_COUNT, HEAD_COUNT, CACHE_LENGTH), jnp.float32, math.log(0.5), math.log(2.0)))
    block_count = CACHE_LENGTH // POS_DEV
    block_multiplier = jnp.exp(jax.random.uniform(every_key[4], (1, HEAD_COUNT, block_count, 1), jnp.float32, math.log(0.4), math.log(2.5)))
    block_multiplier = jnp.broadcast_to(block_multiplier, (1, HEAD_COUNT, block_count, POS_DEV)).reshape(1, HEAD_COUNT, CACHE_LENGTH)
    spike_position = jax.random.randint(every_key[5], (SEQUENCE_COUNT, HEAD_COUNT, 3, 1), 0, CACHE_LENGTH)
    spike_penalty = jnp.log(jax.random.uniform(every_key[6], (SEQUENCE_COUNT, HEAD_COUNT, 3, 1), jnp.float32, 0.5, 0.8))
    cache_positions = jnp.arange(CACHE_LENGTH, dtype=jnp.int32)
    spike_events = jnp.sum(jnp.where(cache_positions[None, None, None, :] == spike_position, spike_penalty, 0.0), axis=2)
    gate_logarithms = spike_events - learning_rate * jaggedness * block_multiplier
    suffix_sum = jnp.flip(jnp.cumsum(jnp.flip(gate_logarithms, 2), axis=2), 2)
    return suffix_sum - gate_logarithms


def shard_levels(own_key, extent, cuts, least, high):
    factor_of = 1.0
    for dim, shards_of in cuts:
        steps = jax.random.uniform(jax.random.fold_in(jax.random.fold_in(own_key, 6), dim), (shards_of,), jnp.float32, least / len(cuts), high / len(cuts))
        factor_of = factor_of * jnp.repeat(jnp.exp(steps), extent[dim] // shards_of).reshape((-1,) + (1,) * (len(extent) - 1 - dim))
    return factor_of


def profile(amount, total, bound, skew):
    portions = [(1 << 20) // math.isqrt(grade ** skew) + 1 for grade in range(2, amount + 1)]
    rest, given = total - bound - (amount - 1), [1] * (amount - 1)
    while rest > 0:
        movable = [i for i in range(amount - 1) if given[i] < bound]
        whole, budget = sum([portions[i] for i in movable]), rest
        for i in movable:
            extra = min(bound - given[i], max(1, budget * portions[i] // whole), rest)
            given[i] = given[i] + extra
            rest = rest - extra
    return np.array([bound] + given)


def ragged(stream_key, count, total, reach, slope):
    if count == 2:
        one = jax.random.randint(stream_key, (), max(1, total - reach), min(reach, total - 1) + 1)
        return jnp.stack([one, total - one])
    tallies = jnp.asarray(profile(count, total, reach, slope), jnp.int32)
    couples = (count - 1) // 2
    source_of, receiver = tallies[1:1 + 2 * couples:2], tallies[2:2 + 2 * couples:2]
    slack = jnp.minimum(source_of - 1, reach - receiver)
    moved = jax.random.randint(jax.random.fold_in(stream_key, 1), (couples,), 0, 1 << 20) % (slack + 1)
    tallies = tallies.at[1:1 + 2 * couples:2].set(source_of - moved).at[2:2 + 2 * couples:2].set(receiver + moved)
    return tallies[jax.random.permutation(jax.random.fold_in(stream_key, 2), count)]


def noise(key, dims, spread, bound, shards=(), kind=jnp.bfloat16):
    entries = spread * jax.random.normal(key, dims, jnp.float32)
    if shards:
        entries = entries * shard_levels(key, dims, shards, -0.22, 0.18)
    return jnp.clip(entries, -bound, bound).astype(kind)


def setup_inputs(seed: int = 0) -> dict:
    splits = jax.random.split(jax.random.key(seed), 16)
    stream = draw_stream(jax.random.fold_in(splits[15], 71), 0)
    gain_in = jnp.clip(1.0 + 0.18 * jax.random.normal(splits[1], (D,), jnp.float32), 0.099609375, 1.8984375).astype(jnp.bfloat16)
    w_query = noise(splits[2], (D, HW), D ** -0.5, 0.09375, ((0, 64), (1, 8)))
    w_key = noise(splits[3], (D, HW), D ** -0.5, 0.09375, ((0, 64), (1, 8)))
    w_value = noise(splits[4], (D, HW), D ** -0.5, 0.09375, ((0, 64), (1, 8)))
    w_forget = noise(splits[5], (D, HEAD_COUNT), D ** -0.5, 0.09375)
    keys_cache = draw_keys_cache(jax.random.fold_in(splits[15], 71), 0)
    values_cache = noise(splits[7], (SEQUENCE_COUNT, HEAD_COUNT, CACHE_LENGTH, HEAD_WIDTH), 1.0, 6.0, ((1, 8), (2, 64)))
    decay_cache = draw_decay_cache(jax.random.fold_in(splits[15], 71), 0)
    lengths = ragged(splits[9], SEQUENCE_COUNT, SEQUENCE_COUNT * CACHE_LENGTH * 2 // 5 + SEQUENCE_COUNT, CACHE_LENGTH, 2).astype(jnp.int32)
    gain_att = jnp.clip(1.0 + 0.18 * jax.random.normal(splits[10], (HW,), jnp.float32), 0.099609375, 1.8984375).astype(jnp.bfloat16)
    w_out = noise(splits[11], (HW, D), HW ** -0.5, 0.125, ((0, 8), (1, 64)))
    gain_mlp = jnp.clip(1.0 + 0.18 * jax.random.normal(splits[12], (D,), jnp.float32), 0.099609375, 1.8984375).astype(jnp.bfloat16)
    w_up = noise(splits[13], (D, FF), D ** -0.5, 0.09375, ((0, 64), (1, 8)))
    w_down = noise(splits[14], (FF, D), FF ** -0.5, 0.046875, ((0, 8), (1, 64)))
    return {"stream": stream, "gain_in": gain_in, "w_query": w_query, "w_key": w_key, "w_value": w_value, "w_forget": w_forget, "keys_cache": keys_cache, "values_cache": values_cache, "decay_cache": decay_cache, "lengths": lengths, "gain_att": gain_att, "w_out": w_out, "gain_mlp": gain_mlp, "w_up": w_up, "w_down": w_down}


norm_eps = 1e-06
masked_score = -1e+30

def head_blocks(head_index, queries, forget, keys_cache, values_cache, decay_cache, lengths):
    block_count = CACHE_LENGTH // POS_DEV
    head_queries = lax.dynamic_index_in_dim(queries, head_index, 1, False).astype(jnp.float32)
    head_keys = lax.dynamic_index_in_dim(keys_cache, head_index, 1, False).astype(jnp.float32)
    value_head = lax.dynamic_index_in_dim(values_cache, head_index, 1, False).astype(jnp.float32)
    decay_head = lax.dynamic_index_in_dim(decay_cache, head_index, 1, False)
    forget_head = lax.dynamic_index_in_dim(forget, head_index, 1, False)
    attention_logits = jnp.einsum('tk,txk->tx', head_queries, head_keys) * (1.0 / math.sqrt(HEAD_WIDTH))
    attention_logits = attention_logits + forget_head[:, None] + decay_head
    attention_logits = attention_logits.reshape(SEQUENCE_COUNT, block_count, POS_DEV)
    cache_positions = jnp.arange(CACHE_LENGTH, dtype=jnp.int32).reshape(block_count, POS_DEV)
    live_mask = cache_positions[None] < lengths.astype(jnp.int32)[:, None, None]
    attention_logits = jnp.where(live_mask, attention_logits, masked_score)
    block_peak = lax.optimization_barrier(jnp.max(attention_logits, axis=2))
    weights = jnp.where(live_mask, jnp.exp(attention_logits - block_peak[..., None]), 0.0)
    block_total = lax.optimization_barrier(jnp.sum(weights, axis=2))
    rounded = lax.optimization_barrier(weights.astype(jnp.bfloat16)).astype(jnp.float32)
    block_out = jnp.einsum('sbp,sbpd->sbd', rounded, value_head.reshape(SEQUENCE_COUNT, block_count, POS_DEV, HEAD_WIDTH))
    return (block_peak, block_total, block_out)

def reference(stream, gain_in, w_query, w_key, w_value, w_forget, keys_cache, values_cache, decay_cache, lengths, gain_att, w_out, gain_mlp, w_up, w_down):
    score_scale = 1.0 / math.sqrt(HEAD_WIDTH)
    stream_float = stream.astype(jnp.float32)
    scaled = (stream_float * gain_in.astype(jnp.float32)).astype(jnp.bfloat16)
    scale_in = lax.rsqrt(lax.optimization_barrier(jnp.mean(stream_float * stream_float, axis=1)) + norm_eps)[:, None]
    queries = (jnp.dot(scaled, w_query, preferred_element_type=jnp.float32) * scale_in).astype(jnp.bfloat16).reshape(SEQUENCE_COUNT, HEAD_COUNT, HEAD_WIDTH)
    key_new = (jnp.dot(scaled, w_key, preferred_element_type=jnp.float32) * scale_in).astype(jnp.bfloat16).reshape(SEQUENCE_COUNT, HEAD_COUNT, HEAD_WIDTH)
    value_new = (jnp.dot(scaled, w_value, preferred_element_type=jnp.float32) * scale_in).astype(jnp.bfloat16).reshape(SEQUENCE_COUNT, HEAD_COUNT, HEAD_WIDTH)
    forget = jax.nn.log_sigmoid(jnp.dot(scaled, w_forget, preferred_element_type=jnp.float32) * scale_in)
    block_peaks, totals, block_outs = lax.map(lambda head_index: head_blocks(head_index, queries, forget, keys_cache, values_cache, decay_cache, lengths), jnp.arange(HEAD_COUNT, dtype=jnp.int32))
    block_peaks = jnp.transpose(block_peaks, (1, 0, 2))
    totals = jnp.transpose(totals, (1, 0, 2))
    block_outs = jnp.transpose(block_outs, (1, 0, 2, 3))
    own_score = lax.optimization_barrier(jnp.sum(queries.astype(jnp.float32) * key_new.astype(jnp.float32), axis=2)) * score_scale
    top_score = jnp.maximum(lax.optimization_barrier(jnp.max(block_peaks, axis=2)), own_score)
    block_weight = jnp.exp(block_peaks - top_score[..., None])
    own_weight = jnp.exp(own_score - top_score)
    numerator = lax.optimization_barrier(jnp.sum(block_weight[..., None] * block_outs, axis=2)) + own_weight[..., None] * value_new.astype(jnp.float32)
    denominator = lax.optimization_barrier(jnp.sum(block_weight * totals, axis=2)) + own_weight
    attended = (numerator / denominator[..., None]).reshape(SEQUENCE_COUNT, HW)
    scale_att = lax.rsqrt(lax.optimization_barrier(jnp.mean(attended * attended, axis=1)) + norm_eps)[:, None]
    attended_in = (attended * gain_att.astype(jnp.float32)).astype(jnp.bfloat16)
    residual = (stream_float + scale_att * jnp.dot(attended_in, w_out, preferred_element_type=jnp.float32)).astype(jnp.bfloat16)
    residual_float = residual.astype(jnp.float32)
    mixer_in = (residual_float * gain_mlp.astype(jnp.float32)).astype(jnp.bfloat16)
    scale_mixer = lax.rsqrt(lax.optimization_barrier(jnp.mean(residual_float * residual_float, axis=1)) + norm_eps)[:, None]
    hidden = jnp.square(jax.nn.relu(jnp.dot(mixer_in, w_up, preferred_element_type=jnp.float32) * scale_mixer)).astype(jnp.bfloat16)
    return (residual_float + jnp.dot(hidden, w_down, preferred_element_type=jnp.float32)).astype(jnp.bfloat16)
```

```python
import math

import jax
import jax.numpy as jnp
from jax import lax
from jax.experimental import pallas as pl
from jax.experimental.pallas import tpu as pltpu
from jax.sharding import Mesh
from jax.sharding import PartitionSpec as P

KV = ("z", "y")
norm_eps = 1e-06
masked_score = -1e30
F32 = jnp.float32
BF16 = jnp.bfloat16
WIDTH = 4096
HEADS_WIDTH = 2048


def swap(value, axis):
    return lax.all_to_all(value, axis, split_axis=0, concat_axis=0, tiled=True)


def dot(a, b):
    return jnp.dot(a, b, preferred_element_type=F32)


def dot_nt(a, b):
    return lax.dot_general(a, b, (((1,), (1,)), ((), ())), preferred_element_type=F32)


def lanes(rows):
    return lax.broadcasted_iota(jnp.int32, (rows, 128), 1)


def row_is(count, index):
    return lax.broadcasted_iota(jnp.int32, (count, 1), 0) == index


def high(value):
    return value.astype(BF16).astype(F32)


def columns(values):
    lane = lanes(values[0].shape[0])
    tile = jnp.zeros(lane.shape, F32)
    for k, value in enumerate(values):
        tile = jnp.where(lane == k, value, tile)
    return tile


def project(stream, gain_in, gain_mlp, w_query, w_key, w_value, w_forget, out, gate_rows, sem):
    kv = lax.axis_index("z") * 4 + lax.axis_index("y")
    head = lax.axis_index("tp") * 2
    start = pl.multiple_of((kv // 2) * 128, 128)
    copy = pltpu.make_async_copy(w_forget.at[:, pl.ds(start, 128)], gate_rows, sem)
    copy.start()
    x = stream[...].astype(F32)
    scaled = (x * gain_in[...].astype(F32)).astype(BF16)
    squares = jnp.sum(x * x, axis=1, keepdims=True)
    for k, w in enumerate((w_query, w_key, w_value)):
        part = dot(scaled, w[...])
        for y in range(4):
            for h in range(2):
                out[y, k * 16 + h * 8 : k * 16 + h * 8 + 8, :] = part[y * 8 : y * 8 + 8, h * 128 : h * 128 + 128]
    copy.wait()
    wide = jnp.concatenate([scaled, scaled], axis=1)
    wide = jnp.where(lanes(32) // 64 == kv % 2, wide.astype(F32), 0.0).astype(BF16)
    gates = dot_nt(wide, gate_rows[...])
    column = lax.broadcasted_iota(jnp.int32, gates.shape, 1)
    first = jnp.sum(jnp.where(column == head, gates, 0.0), axis=1, keepdims=True)
    second = jnp.sum(jnp.where(column == head + 1, gates, 0.0), axis=1, keepdims=True)
    gain = gain_mlp[...].astype(F32)
    gain = jnp.broadcast_to(jnp.concatenate([gain, gain], axis=1), (32, 128))
    extra = jnp.where(lanes(32) < 64, columns([squares, first, second]), gain)
    twice = jnp.concatenate([x, x], axis=1)
    for y in range(4):
        out[y, 48:56, :] = extra[y * 8 : y * 8 + 8]
        out[y, 56:64, :] = twice[y * 8 : y * 8 + 8]


def spread_rows(got, out, stream_all, gain_all):
    total = got[0, 0:56] + got[1, 0:56] + got[2, 0:56] + got[3, 0:56]
    q = total[0:16].astype(BF16)
    x = jnp.where(lanes(8) < 3, total[48:56], 0.0)
    one = high(x)
    two = high(x - one)
    three = high(x - one - two)
    extra = one + pltpu.roll(two, 4, 1) + pltpu.roll(three, 8, 1)
    row = lax.broadcasted_iota(jnp.int32, (8, 128), 0)
    for p in range(16):
        k = total[16 + p : 17 + p]
        v = total[32 + p : 33 + p]
        own = jnp.where(row == 0, k, jnp.where(row == 1, v, 0.0))
        out[p, 0:16, :] = q
        out[p, 16:32, :] = jnp.concatenate([extra, own], axis=0).astype(BF16)
    left = lanes(8) < 64
    for k in range(2):
        stream_all[k] = jnp.where(left, got[2 * k, 56:64], got[2 * k + 1, 56:64])
        gain_all[k] = jnp.where(left, pltpu.roll(got[2 * k, 48:56], 64, 1), got[2 * k + 1, 48:56])


def finish_rows(got, w_out, out, own_out):
    z = lax.axis_index("z")
    total = got[0].astype(F32)
    for k in range(1, 16):
        total = total + got[k].astype(F32)
    x = total[16:24]
    x = x + pltpu.roll(x, 124, 1) + pltpu.roll(x, 120, 1)
    scale = lax.rsqrt(x[:, 0:1] / WIDTH + norm_eps)
    scale = jnp.concatenate([scale, scale], axis=0)
    gate = jnp.concatenate([x[:, 1:2], x[:, 2:3]], axis=0) * scale
    q = (total[0:16] * scale).astype(BF16)
    mine = row_is(16, z)
    scale_z = jnp.sum(jnp.where(mine, scale, 0.0), axis=0, keepdims=True)
    gate_z = jnp.sum(jnp.where(mine, gate, 0.0), axis=0, keepdims=True)
    k = high(total[24:25] * scale_z)
    v = high(total[25:26] * scale_z)
    q_z = jnp.sum(jnp.where(mine, q.astype(F32), 0.0), axis=0, keepdims=True)
    own = jnp.sum(q_z * k, axis=1, keepdims=True) * (1.0 / math.sqrt(128))
    own = own + jnp.maximum(-gate_z, 0.0) + jnp.log1p(jnp.exp(-jnp.abs(gate_z)))
    row = lax.broadcasted_iota(jnp.int32, (8, 128), 0)
    own_out[...] = jnp.where(row == 0, own, v)
    w = w_out[...]
    for y in range(4):
        out[y, 0:16, :] = q
        out[y, 16:80, :] = w[:, 0:128]
        out[y, 80:144, :] = w[:, 128:256]


def attend(q, keys, values, decay, lengths, first):
    q = q.reshape(4, 2, 8, 128).swapaxes(1, 2).reshape(32, 2, 128)
    s = jnp.einsum("shd,shpd->shp", q, keys, preferred_element_type=F32)
    s = s * (1.0 / math.sqrt(128)) + decay
    live = (first + lax.iota(jnp.int32, 128)[None, :] < lengths[:, None])[:, None, :]
    s = jnp.where(live, s, masked_score)
    peak = jnp.max(s, axis=2, keepdims=True)
    probs = jnp.where(live, jnp.exp(s - peak), 0.0)
    total = jnp.sum(probs, axis=2, keepdims=True)
    out = jnp.einsum("shp,shpd->shd", probs.astype(BF16), values, preferred_element_type=F32)
    lane = lax.broadcasted_iota(jnp.int32, (32, 2, 128), 2)
    extra = jnp.where(lane == 0, peak, total)
    both = jnp.stack([out, extra]).reshape(2, 4, 8, 2, 128)
    return both.transpose(1, 0, 3, 2, 4).reshape(4, 32, 128)


def merge_blocks(got, own, out):
    z = lax.axis_index("z")
    peaks = [got[k, 16:32, 0:1] for k in range(4)]
    totals = [got[k, 16:32, 1:2] for k in range(4)]
    mine = row_is(16, z)
    own_peak = jnp.where(mine, own[0:1, 0:1], masked_score)
    top = own_peak
    for peak in peaks:
        top = jnp.maximum(top, peak)
    own_weight = jnp.where(mine, jnp.exp(own_peak - top), 0.0)
    total = own_weight
    merged = own_weight * own[1:2, :]
    for k in range(4):
        weight = jnp.exp(peaks[k] - top)
        total = total + weight * totals[k]
        merged = merged + weight * got[k, 0:16]
    one = high(top)
    two = high(top - one)
    three = top - one - two
    four = high(total)
    five = total - four
    parts = []
    for h in range(2):
        for value in (one, two, three, four, five):
            parts.append(value[h * 8 : h * 8 + 8])
    extra = columns(parts).astype(BF16)
    merged = merged.astype(BF16)
    for k in range(16):
        out[k, 0:16, :] = merged
        out[k, 16:24, :] = extra


def project_out(got, w_all, gain_att, out):
    gain = gain_att[...].astype(F32)
    squares = jnp.zeros((8, 1), F32)
    part = jnp.zeros((8, 256), F32)
    extras = [got[k, 16:24, :].astype(F32) for k in range(16)]
    for h in range(2):
        c = h * 5
        peaks = [e[:, c : c + 1] + e[:, c + 1 : c + 2] + e[:, c + 2 : c + 3] for e in extras]
        top = peaks[0]
        for peak in peaks[1:]:
            top = jnp.maximum(top, peak)
        total = jnp.zeros((8, 1), F32)
        merged = jnp.zeros((8, 128), F32)
        for k in range(16):
            weight = jnp.exp(peaks[k] - top)
            total = total + weight * (extras[k][:, c + 3 : c + 4] + extras[k][:, c + 4 : c + 5])
            merged = merged + weight * got[k, 0:16, :].astype(F32)[h * 8 : h * 8 + 8]
        attended = merged / total
        squares = squares + jnp.sum(attended * attended, axis=1, keepdims=True)
        attended_in = (attended * gain[:, h * 128 : h * 128 + 128]).astype(BF16)
        w = jnp.concatenate([w_all[y, 16 + h * 64 : 80 + h * 64, :] for y in range(4)], axis=0)
        part = part + dot_nt(attended_in, w)
    extra = columns([squares])
    for k in range(8):
        out[k, 0:8, :] = part[:, 0:128]
        out[k, 8:16, :] = part[:, 128:256]
        out[k, 16:24, :] = extra


def mix_up(got, stream_all, gain_all, w0, w1, w2, w3, out, residual_out, halves):
    y = lax.axis_index("y")
    total = got[0]
    for k in range(1, 8):
        total = total + got[k]
    scale = lax.rsqrt(total[16:24, 0:1] / HEADS_WIDTH + norm_eps)
    squares = jnp.zeros((8, 1), F32)
    for k in range(2):
        residual = high(stream_all[k] + scale * total[k * 8 : k * 8 + 8])
        squares = squares + jnp.sum(residual * residual, axis=1, keepdims=True)
        mixer_in = high(residual * gain_all[k])
        halves[2 * k] = mixer_in
        halves[2 * k + 1] = pltpu.roll(mixer_in, 64, 1)
        residual_out[2 * k] = residual
        residual_out[2 * k + 1] = pltpu.roll(residual, 64, 1)
    up = jnp.zeros((8, 2048), F32)
    for d, w in enumerate((w0, w1, w2, w3)):
        lhs = halves[(y + 4 - d) % 4][:, 0:64].astype(BF16)
        up = up + dot(lhs, w[...])
    one = high(squares)
    two = high(squares - one)
    extra = columns([one, two, squares - one - two])
    for k in range(16):
        both = jnp.concatenate([up[:, k * 128 : k * 128 + 128], extra], axis=0)
        out[k] = both.astype(BF16)


def activate(got, out):
    total = got[0].astype(F32)
    for k in range(1, 16):
        total = total + got[k].astype(F32)
    squares = total[8:16, 0:1] + total[8:16, 1:2] + total[8:16, 2:3]
    scale = lax.rsqrt(squares / WIDTH + norm_eps)
    hidden = jnp.square(jnp.maximum(total[0:8] * scale, 0.0)).astype(BF16)
    for k in range(16):
        out[k] = hidden


def mix_down(got, residual, w0, w1, w2, w3, out):
    y = lax.axis_index("y")
    t = lax.axis_index("tp")
    hidden = jnp.concatenate([got[k] for k in range(16)], axis=1)
    for d, w in enumerate((w0, w1, w2, w3)):
        source = (y + 4 - d) % 4
        part = dot_nt(hidden, w[...])
        part = jnp.concatenate([part, part], axis=1)
        part = part + jnp.where(t == 0, residual[source], 0.0)
        for k in range(8):
            out[source * 8 + k] = part


def finish(got, out):
    for y in range(4):
        total = got[y * 8]
        for k in range(1, 8):
            total = total + got[y * 8 + k]
        out[y * 8 : y * 8 + 8, :] = total[:, 0:64].astype(BF16)


def call(kernel, outs, *args, anywhere=(), scratch=()):
    specs = [
        pl.BlockSpec(memory_space=pl.ANY) if k in anywhere else pl.BlockSpec(memory_space=pltpu.VMEM)
        for k in range(len(args))
    ]
    shapes = [jax.ShapeDtypeStruct(s, d) for s, d in outs]
    found = pl.pallas_call(
        kernel,
        out_shape=shapes,
        in_specs=specs,
        out_specs=[pl.BlockSpec(memory_space=pltpu.VMEM) for _ in shapes],
        scratch_shapes=list(scratch),
        name=kernel.__name__,
    )(*args)
    return found if len(shapes) > 1 else found[0]


def around(value):
    n = lax.axis_size("y")
    moved = [lax.ppermute(value, "y", [(k, (k + d) % n) for k in range(n)]) for d in range(1, n)]
    return [value, *moved]


def per_device(
    stream,
    gain_in,
    w_query,
    w_key,
    w_value,
    w_forget,
    keys_cache,
    values_cache,
    decay_cache,
    lengths,
    gain_att,
    w_out,
    gain_mlp,
    w_up,
    w_down,
):
    kv = lax.axis_index(KV)
    lines = call(
        project,
        [((4, 64, 128), F32)],
        stream,
        gain_in.reshape(1, 64),
        gain_mlp.reshape(1, 64),
        w_query,
        w_key,
        w_value,
        w_forget.T,
        anywhere=(6,),
        scratch=(pltpu.VMEM((16, 128), BF16), pltpu.SemaphoreType.DMA),
    )
    got = swap(lines, "y")
    lines, stream_all, gain_all = call(
        spread_rows, [((16, 32, 128), BF16), ((2, 8, 128), F32), ((2, 8, 128), F32)], got
    )
    lines, w_up, w_down = lax.optimization_barrier((lines, w_up, w_down))
    got = swap(lines, "z")
    ups = around(w_up)
    downs = around(w_down.T)
    lines, own = call(finish_rows, [((4, 144, 128), BF16), ((8, 128), F32)], got, w_out.T)
    w_all = swap(lines, "y")
    got = swap(attend(w_all[:, 0:16], keys_cache, values_cache, decay_cache, lengths, kv * 128), "y")
    lines = call(merge_blocks, [((16, 24, 128), BF16)], got, own)
    got = swap(lines, "z")
    lines = call(project_out, [((8, 24, 128), F32)], got, w_all, gain_att.reshape(1, 256))
    got = swap(lines, "tp")
    lines, residual = call(
        mix_up,
        [((16, 16, 128), BF16), ((4, 8, 128), F32)],
        got,
        stream_all,
        gain_all,
        *ups,
        scratch=(pltpu.VMEM((4, 8, 128), F32),),
    )
    got = swap(lines, "z")
    got = swap(call(activate, [((16, 8, 128), BF16)], got), "z")
    lines = call(mix_down, [((32, 8, 128), F32)], got, residual, *downs)
    got = swap(lines, ("y", "tp"))
    return call(finish, [((32, 64), BF16)], got)


def solution(mesh):
    split = Mesh(mesh.devices.reshape(16, 4, mesh.shape["tp"]), ("z", "y", "tp"))
    return jax.shard_map(
        per_device,
        mesh=split,
        in_specs=(
            P(None, KV),
            P(KV),
            P(KV, "tp"),
            P(KV, "tp"),
            P(KV, "tp"),
            P(),
            P(None, "tp", KV, None),
            P(None, "tp", KV, None),
            P(None, "tp", KV),
            P(),
            P("tp"),
            P("tp", KV),
            P(KV),
            P(KV, "tp"),
            P("tp", KV),
        ),
        out_specs=P(None, KV),
        check_vma=False,
    )
```

```python
import math

import jax
import jax.numpy as jnp
from jax import lax
from jax.experimental import pallas as pl
from jax.experimental.pallas import tpu as pltpu
from jax.sharding import Mesh
from jax.sharding import PartitionSpec as P

KV = ("z", "y")
norm_eps = 1e-06
masked_score = -1e30
F32 = jnp.float32
BF16 = jnp.bfloat16
WIDTH = 4096
HEADS_WIDTH = 2048


def swap(value, axis):
    return lax.all_to_all(value, axis, split_axis=0, concat_axis=0, tiled=True)


def dot(a, b):
    return jnp.dot(a, b, preferred_element_type=F32)


def dot_nt(a, b):
    return lax.dot_general(a, b, (((1,), (1,)), ((), ())), preferred_element_type=F32)


def lanes(rows):
    return lax.broadcasted_iota(jnp.int32, (rows, 128), 1)


def row_is(count, index):
    return lax.broadcasted_iota(jnp.int32, (count, 1), 0) == index


def high(value):
    return value.astype(BF16).astype(F32)


def columns(values):
    lane = lanes(values[0].shape[0])
    tile = jnp.zeros(lane.shape, F32)
    for k, value in enumerate(values):
        tile = jnp.where(lane == k, value, tile)
    return tile


def project(stream, gain_in, gain_mlp, w_query, w_key, w_value, w_forget, out, gate_rows, sem):
    kv = lax.axis_index("z") * 4 + lax.axis_index("y")
    head = lax.axis_index("tp") * 2
    start = pl.multiple_of((kv // 2) * 128, 128)
    copy = pltpu.make_async_copy(w_forget.at[:, pl.ds(start, 128)], gate_rows, sem)
    copy.start()
    x = stream[...].astype(F32)
    scaled = (x * gain_in[...].astype(F32)).astype(BF16)
    squares = jnp.sum(x * x, axis=1, keepdims=True)
    for k, w in enumerate((w_query, w_key, w_value)):
        part = dot(scaled, w[...])
        for y in range(4):
            for h in range(2):
                out[y, k * 16 + h * 8 : k * 16 + h * 8 + 8, :] = part[y * 8 : y * 8 + 8, h * 128 : h * 128 + 128]
    copy.wait()
    wide = jnp.concatenate([scaled, scaled], axis=1)
    wide = jnp.where(lanes(32) // 64 == kv % 2, wide.astype(F32), 0.0).astype(BF16)
    gates = dot_nt(wide, gate_rows[...])
    column = lax.broadcasted_iota(jnp.int32, gates.shape, 1)
    first = jnp.sum(jnp.where(column == head, gates, 0.0), axis=1, keepdims=True)
    second = jnp.sum(jnp.where(column == head + 1, gates, 0.0), axis=1, keepdims=True)
    gain = gain_mlp[...].astype(F32)
    gain = jnp.broadcast_to(jnp.concatenate([gain, gain], axis=1), (32, 128))
    extra = jnp.where(lanes(32) < 64, columns([squares, first, second]), gain)
    twice = jnp.concatenate([x, x], axis=1)
    for y in range(4):
        out[y, 48:56, :] = extra[y * 8 : y * 8 + 8]
        out[y, 56:64, :] = twice[y * 8 : y * 8 + 8]


def spread_rows(got, out, stream_all, gain_all):
    total = got[0, 0:56] + got[1, 0:56] + got[2, 0:56] + got[3, 0:56]
    q = total[0:16].astype(BF16)
    x = jnp.where(lanes(8) < 3, total[48:56], 0.0)
    one = high(x)
    two = high(x - one)
    three = high(x - one - two)
    extra = one + pltpu.roll(two, 4, 1) + pltpu.roll(three, 8, 1)
    row = lax.broadcasted_iota(jnp.int32, (8, 128), 0)
    for p in range(16):
        k = total[16 + p : 17 + p]
        v = total[32 + p : 33 + p]
        own = jnp.where(row == 0, k, jnp.where(row == 1, v, 0.0))
        out[p, 0:16, :] = q
        out[p, 16:32, :] = jnp.concatenate([extra, own], axis=0).astype(BF16)
    left = lanes(8) < 64
    for k in range(2):
        stream_all[k] = jnp.where(left, got[2 * k, 56:64], got[2 * k + 1, 56:64])
        gain_all[k] = jnp.where(left, pltpu.roll(got[2 * k, 48:56], 64, 1), got[2 * k + 1, 48:56])


def finish_rows(got, w_out, out, own_out):
    z = lax.axis_index("z")
    total = got[0].astype(F32)
    for k in range(1, 16):
        total = total + got[k].astype(F32)
    x = total[16:24]
    x = x + pltpu.roll(x, 124, 1) + pltpu.roll(x, 120, 1)
    scale = lax.rsqrt(x[:, 0:1] / WIDTH + norm_eps)
    scale = jnp.concatenate([scale, scale], axis=0)
    gate = jnp.concatenate([x[:, 1:2], x[:, 2:3]], axis=0) * scale
    q = (total[0:16] * scale).astype(BF16)
    mine = row_is(16, z)
    scale_z = jnp.sum(jnp.where(mine, scale, 0.0), axis=0, keepdims=True)
    gate_z = jnp.sum(jnp.where(mine, gate, 0.0), axis=0, keepdims=True)
    k = high(total[24:25] * scale_z)
    v = high(total[25:26] * scale_z)
    q_z = jnp.sum(jnp.where(mine, q.astype(F32), 0.0), axis=0, keepdims=True)
    own = jnp.sum(q_z * k, axis=1, keepdims=True) * (1.0 / math.sqrt(128))
    own = own + jnp.maximum(-gate_z, 0.0) + jnp.log1p(jnp.exp(-jnp.abs(gate_z)))
    row = lax.broadcasted_iota(jnp.int32, (8, 128), 0)
    own_out[...] = jnp.where(row == 0, own, v)
    w = w_out[...]
    for y in range(4):
        out[y, 0:16, :] = q
        out[y, 16:80, :] = w[:, 0:128]
        out[y, 80:144, :] = w[:, 128:256]


def attend(q, keys, values, decay, lengths, first):
    q = q.reshape(4, 2, 8, 128).swapaxes(1, 2).reshape(32, 2, 128)
    s = jnp.einsum("shd,shpd->shp", q, keys, preferred_element_type=F32)
    s = s * (1.0 / math.sqrt(128)) + decay
    live = (first + lax.iota(jnp.int32, 128)[None, :] < lengths[:, None])[:, None, :]
    s = jnp.where(live, s, masked_score)
    peak = jnp.max(s, axis=2, keepdims=True)
    probs = jnp.where(live, jnp.exp(s - peak), 0.0)
    total = jnp.sum(probs, axis=2, keepdims=True)
    out = jnp.einsum("shp,shpd->shd", probs.astype(BF16), values, preferred_element_type=F32)
    lane = lax.broadcasted_iota(jnp.int32, (32, 2, 128), 2)
    extra = jnp.where(lane == 0, peak, total)
    both = jnp.stack([out, extra]).reshape(2, 4, 8, 2, 128)
    return both.transpose(1, 0, 3, 2, 4).reshape(4, 32, 128)


def merge_blocks(got, own, out):
    z = lax.axis_index("z")
    peaks = [got[k, 16:32, 0:1] for k in range(4)]
    totals = [got[k, 16:32, 1:2] for k in range(4)]
    mine = row_is(16, z)
    own_peak = jnp.where(mine, own[0:1, 0:1], masked_score)
    top = own_peak
    for peak in peaks:
        top = jnp.maximum(top, peak)
    own_weight = jnp.where(mine, jnp.exp(own_peak - top), 0.0)
    total = own_weight
    merged = own_weight * own[1:2, :]
    for k in range(4):
        weight = jnp.exp(peaks[k] - top)
        total = total + weight * totals[k]
        merged = merged + weight * got[k, 0:16]
    one = high(top)
    two = high(top - one)
    three = top - one - two
    four = high(total)
    five = total - four
    parts = []
    for h in range(2):
        for value in (one, two, three, four, five):
            parts.append(value[h * 8 : h * 8 + 8])
    extra = columns(parts).astype(BF16)
    merged = merged.astype(BF16)
    for k in range(16):
        out[k, 0:16, :] = merged
        out[k, 16:24, :] = extra


def project_out(got, w_all, gain_att, out):
    gain = gain_att[...].astype(F32)
    squares = jnp.zeros((8, 1), F32)
    part = jnp.zeros((8, 256), F32)
    extras = [got[k, 16:24, :].astype(F32) for k in range(16)]
    for h in range(2):
        c = h * 5
        peaks = [e[:, c : c + 1] + e[:, c + 1 : c + 2] + e[:, c + 2 : c + 3] for e in extras]
        top = peaks[0]
        for peak in peaks[1:]:
            top = jnp.maximum(top, peak)
        total = jnp.zeros((8, 1), F32)
        merged = jnp.zeros((8, 128), F32)
        for k in range(16):
            weight = jnp.exp(peaks[k] - top)
            total = total + weight * (extras[k][:, c + 3 : c + 4] + extras[k][:, c + 4 : c + 5])
            merged = merged + weight * got[k, 0:16, :].astype(F32)[h * 8 : h * 8 + 8]
        attended = merged / total
        squares = squares + jnp.sum(attended * attended, axis=1, keepdims=True)
        attended_in = (attended * gain[:, h * 128 : h * 128 + 128]).astype(BF16)
        w = jnp.concatenate([w_all[y, 16 + h * 64 : 80 + h * 64, :] for y in range(4)], axis=0)
        part = part + dot_nt(attended_in, w)
    extra = columns([squares])
    for k in range(8):
        out[k, 0:8, :] = part[:, 0:128]
        out[k, 8:16, :] = part[:, 128:256]
        out[k, 16:24, :] = extra


def mix_up(got, stream_all, gain_all, w0, w1, w2, w3, out, residual_out, halves):
    y = lax.axis_index("y")
    total = got[0]
    for k in range(1, 8):
        total = total + got[k]
    scale = lax.rsqrt(total[16:24, 0:1] / HEADS_WIDTH + norm_eps)
    squares = jnp.zeros((8, 1), F32)
    for k in range(2):
        residual = high(stream_all[k] + scale * total[k * 8 : k * 8 + 8])
        squares = squares + jnp.sum(residual * residual, axis=1, keepdims=True)
        mixer_in = high(residual * gain_all[k])
        halves[2 * k] = mixer_in
        halves[2 * k + 1] = pltpu.roll(mixer_in, 64, 1)
        residual_out[2 * k] = residual
        residual_out[2 * k + 1] = pltpu.roll(residual, 64, 1)
    up = jnp.zeros((8, 2048), F32)
    for d, w in enumerate((w0, w1, w2, w3)):
        lhs = halves[(y + 4 - d) % 4][:, 0:64].astype(BF16)
        up = up + dot(lhs, w[0:64, :])
    one = high(squares)
    two = high(squares - one)
    extra = columns([one, two, squares - one - two])
    for k in range(16):
        both = jnp.concatenate([up[:, k * 128 : k * 128 + 128], extra], axis=0)
        out[k] = both.astype(BF16)


def activate(got, out):
    total = got[0].astype(F32)
    for k in range(1, 16):
        total = total + got[k].astype(F32)
    squares = total[8:16, 0:1] + total[8:16, 1:2] + total[8:16, 2:3]
    scale = lax.rsqrt(squares / WIDTH + norm_eps)
    hidden = jnp.square(jnp.maximum(total[0:8] * scale, 0.0)).astype(BF16)
    for k in range(16):
        out[k] = hidden


def mix_down(got, residual, w0, w1, w2, w3, out):
    y = lax.axis_index("y")
    t = lax.axis_index("tp")
    hidden = jnp.concatenate([got[k] for k in range(16)], axis=1)
    for d, w in enumerate((w0, w1, w2, w3)):
        source = (y + 4 - d) % 4
        part = dot_nt(hidden, w[64:128, :])
        part = jnp.concatenate([part, part], axis=1)
        part = part + jnp.where(t == 0, residual[source], 0.0)
        for k in range(8):
            out[source * 8 + k] = part


def finish(got, out):
    for y in range(4):
        total = got[y * 8]
        for k in range(1, 8):
            total = total + got[y * 8 + k]
        out[y * 8 : y * 8 + 8, :] = total[:, 0:64].astype(BF16)


def call(kernel, outs, *args, near=(0,), anywhere=(), scratch=()):
    specs = [
        pl.BlockSpec(memory_space=pl.ANY) if k in anywhere else pl.BlockSpec(memory_space=pltpu.VMEM)
        for k in range(len(args))
    ]
    args = [pltpu.with_memory_space_constraint(a, pltpu.VMEM) if k in near else a for k, a in enumerate(args)]
    shapes = [pltpu.VMEM(s, d) for s, d in outs]
    found = pl.pallas_call(
        kernel,
        out_shape=shapes,
        in_specs=specs,
        out_specs=[pl.BlockSpec(memory_space=pltpu.VMEM) for _ in shapes],
        scratch_shapes=list(scratch),
    )(*args)
    return found if len(shapes) > 1 else found[0]


def turned(value, d):
    n = lax.axis_size("y")
    return lax.ppermute(value, "y", [(k, (k + d) % n) for k in range(n)])


def layer(
    stream,
    gain_in,
    w_query,
    w_key,
    w_value,
    w_forget,
    keys_cache,
    values_cache,
    decay_cache,
    lengths,
    gain_att,
    w_out,
    gain_mlp,
    w_up,
    w_down,
):
    kv = lax.axis_index(KV)
    lines = call(
        project,
        [((4, 64, 128), F32)],
        stream,
        gain_in.reshape(1, 64),
        gain_mlp.reshape(1, 64),
        w_query,
        w_key,
        w_value,
        w_forget.T,
        near=(),
        anywhere=(6,),
        scratch=(pltpu.VMEM((16, 128), BF16), pltpu.SemaphoreType.DMA),
    )
    got = swap(lines, "y")
    lines, stream_all, gain_all = call(
        spread_rows, [((16, 32, 128), BF16), ((2, 8, 128), F32), ((2, 8, 128), F32)], got
    )
    lines, w_up, w_down = lax.optimization_barrier((lines, w_up, w_down.T))
    got = swap(lines, "z")
    w0 = jnp.concatenate([w_up, w_down], axis=0)
    w1 = turned(w0, 1)
    w3 = turned(w0, 3)
    lines, own = call(finish_rows, [((4, 144, 128), BF16), ((8, 128), F32)], got, w_out.T)
    lines, w1, w3 = lax.optimization_barrier((lines, w1, w3))
    w_all = swap(lines, "y")
    got = swap(attend(w_all[:, 0:16], keys_cache, values_cache, decay_cache, lengths, kv * 128), "y")
    lines = call(merge_blocks, [((16, 24, 128), BF16)], got, own, near=(0, 1))
    lines, w2 = lax.optimization_barrier((lines, w0))
    got = swap(lines, "z")
    w2 = turned(w2, 2)
    lines = call(project_out, [((8, 24, 128), F32)], got, w_all, gain_att.reshape(1, 256), near=(0, 1))
    lines, w2 = lax.optimization_barrier((lines, w2))
    got = swap(lines, "tp")
    lines, residual = call(
        mix_up,
        [((16, 16, 128), BF16), ((4, 8, 128), F32)],
        got,
        stream_all,
        gain_all,
        w0,
        w1,
        w2,
        w3,
        near=tuple(range(7)),
        scratch=(pltpu.VMEM((4, 8, 128), F32),),
    )
    got = swap(lines, "z")
    got = swap(call(activate, [((16, 8, 128), BF16)], got), "z")
    lines = call(mix_down, [((32, 8, 128), F32)], got, residual, w0, w1, w2, w3, near=tuple(range(6)))
    got = swap(lines, ("y", "tp"))
    return call(finish, [((32, 64), BF16)], got)


def solution(mesh):
    split = Mesh(mesh.devices.reshape(16, 4, mesh.shape["tp"]), ("z", "y", "tp"))
    return jax.shard_map(
        layer,
        mesh=split,
        in_specs=(
            P(None, KV),
            P(KV),
            P(KV, "tp"),
            P(KV, "tp"),
            P(KV, "tp"),
            P(),
            P(None, "tp", KV, None),
            P(None, "tp", KV, None),
            P(None, "tp", KV),
            P(),
            P("tp"),
            P("tp", KV),
            P(KV),
            P(KV, "tp"),
            P("tp", KV),
        ),
        out_specs=P(None, KV),
        check_vma=False,
    )
```

```python
import math

import jax
import jax.numpy as jnp
from jax import lax
from jax.experimental import pallas as pl
from jax.experimental.pallas import tpu as pltpu
from jax.sharding import Mesh
from jax.sharding import PartitionSpec as P

KV = ("z", "y")
norm_eps = 1e-06
masked_score = -1e30
F32 = jnp.float32
BF16 = jnp.bfloat16
LIMIT = 8 * 1024 * 1024
WIDTH = 4096
HEADS_WIDTH = 2048


def swap(value, axis):
    return lax.all_to_all(value, axis, split_axis=0, concat_axis=0, tiled=True)


def dot(a, b):
    return jnp.dot(a, b, preferred_element_type=F32)


def dot_nt(a, b):
    return lax.dot_general(a, b, (((1,), (1,)), ((), ())), preferred_element_type=F32)


def lanes(rows):
    return lax.broadcasted_iota(jnp.int32, (rows, 128), 1)


def row_is(count, index):
    return lax.broadcasted_iota(jnp.int32, (count, 1), 0) == index


def high(value):
    return value.astype(BF16).astype(F32)


def columns(values):
    lane = lanes(values[0].shape[0])
    tile = jnp.zeros(lane.shape, F32)
    for k, value in enumerate(values):
        tile = jnp.where(lane == k, value, tile)
    return tile


def project(stream, gain_in, gain_mlp, w_query, w_key, w_value, w_forget, out, gate_rows, sem):
    kv = lax.axis_index("z") * 4 + lax.axis_index("y")
    head = lax.axis_index("tp") * 2
    start = pl.multiple_of((kv // 2) * 128, 128)
    copy = pltpu.make_async_copy(w_forget.at[:, pl.ds(start, 128)], gate_rows, sem)
    copy.start()
    x = stream[...].astype(F32)
    scaled = (x * gain_in[...].astype(F32)).astype(BF16)
    squares = jnp.sum(x * x, axis=1, keepdims=True)
    for k, w in enumerate((w_query, w_key, w_value)):
        part = dot(scaled, w[...])
        for y in range(4):
            for h in range(2):
                out[y, k * 16 + h * 8 : k * 16 + h * 8 + 8, :] = part[y * 8 : y * 8 + 8, h * 128 : h * 128 + 128]
    copy.wait()
    wide = jnp.concatenate([scaled, scaled], axis=1)
    wide = jnp.where(lanes(32) // 64 == kv % 2, wide.astype(F32), 0.0).astype(BF16)
    gates = dot_nt(wide, gate_rows[...])
    column = lax.broadcasted_iota(jnp.int32, gates.shape, 1)
    first = jnp.sum(jnp.where(column == head, gates, 0.0), axis=1, keepdims=True)
    second = jnp.sum(jnp.where(column == head + 1, gates, 0.0), axis=1, keepdims=True)
    gain = gain_mlp[...].astype(F32)
    gain = jnp.broadcast_to(jnp.concatenate([gain, gain], axis=1), (32, 128))
    extra = jnp.where(lanes(32) < 64, columns([squares, first, second]), gain)
    twice = jnp.concatenate([x, x], axis=1)
    for y in range(4):
        out[y, 48:56, :] = extra[y * 8 : y * 8 + 8]
        out[y, 56:64, :] = twice[y * 8 : y * 8 + 8]


def spread_rows(got, out, stream_all, gain_all):
    total = got[0, 0:56] + got[1, 0:56] + got[2, 0:56] + got[3, 0:56]
    q = total[0:16].astype(BF16)
    x = jnp.where(lanes(8) < 3, total[48:56], 0.0)
    one = high(x)
    two = high(x - one)
    three = high(x - one - two)
    extra = one + pltpu.roll(two, 4, 1) + pltpu.roll(three, 8, 1)
    row = lax.broadcasted_iota(jnp.int32, (8, 128), 0)
    for p in range(16):
        k = total[16 + p : 17 + p]
        v = total[32 + p : 33 + p]
        own = jnp.where(row == 0, k, jnp.where(row == 1, v, 0.0))
        out[p, 0:16, :] = q
        out[p, 16:32, :] = jnp.concatenate([extra, own], axis=0).astype(BF16)
    left = lanes(8) < 64
    for k in range(2):
        stream_all[k] = jnp.where(left, got[2 * k, 56:64], got[2 * k + 1, 56:64])
        gain_all[k] = jnp.where(left, pltpu.roll(got[2 * k, 48:56], 64, 1), got[2 * k + 1, 48:56])


def finish_rows(got, w_out, out, own_out):
    z = lax.axis_index("z")
    total = got[0].astype(F32)
    for k in range(1, 16):
        total = total + got[k].astype(F32)
    x = total[16:24]
    x = x + pltpu.roll(x, 124, 1) + pltpu.roll(x, 120, 1)
    scale = lax.rsqrt(x[:, 0:1] / WIDTH + norm_eps)
    scale = jnp.concatenate([scale, scale], axis=0)
    gate = jnp.concatenate([x[:, 1:2], x[:, 2:3]], axis=0) * scale
    q = (total[0:16] * scale).astype(BF16)
    mine = row_is(16, z)
    scale_z = jnp.sum(jnp.where(mine, scale, 0.0), axis=0, keepdims=True)
    gate_z = jnp.sum(jnp.where(mine, gate, 0.0), axis=0, keepdims=True)
    k = high(total[24:25] * scale_z)
    v = high(total[25:26] * scale_z)
    q_z = jnp.sum(jnp.where(mine, q.astype(F32), 0.0), axis=0, keepdims=True)
    own = jnp.sum(q_z * k, axis=1, keepdims=True) * (1.0 / math.sqrt(128))
    own = own + jnp.maximum(-gate_z, 0.0) + jnp.log1p(jnp.exp(-jnp.abs(gate_z)))
    row = lax.broadcasted_iota(jnp.int32, (8, 128), 0)
    own_out[...] = jnp.where(row == 0, own, v)
    w = w_out[...]
    for y in range(4):
        out[y, 0:16, :] = q
        out[y, 16:80, :] = w[:, 0:128]
        out[y, 80:144, :] = w[:, 128:256]


def attend(w_all, keys, values_far, decay, lengths, out, values, sems):
    copies = []
    for y in range(4):
        part = pl.ds(y * 8, 8)
        copies.append(pltpu.make_async_copy(values_far.at[part], values.at[part], sems.at[y]))
        copies[y].start()
    first = (lax.axis_index("z") * 4 + lax.axis_index("y")) * 128
    place = lanes(8) + first
    row = lax.broadcasted_iota(jnp.int32, (8, 128), 0)
    for y in range(4):
        q = w_all[y, 0:16, :]
        every = dot_nt(q, keys[y * 8 : y * 8 + 8].reshape(2048, 128))
        length = jnp.zeros((8, 128), jnp.int32)
        for b in range(8):
            length = jnp.where(row == b, lengths[y * 8 + b], length)
        live = place < length
        probs = []
        for h in range(2):
            s = jnp.zeros((8, 128), F32)
            for b in range(8):
                c = (b * 2 + h) * 128
                s = jnp.where(row == b, every[h * 8 : h * 8 + 8, c : c + 128], s)
            s = s * (1.0 / math.sqrt(128)) + decay[y * 8 : y * 8 + 8, h, :]
            s = jnp.where(live, s, masked_score)
            peak = jnp.max(s, axis=1, keepdims=True)
            p = jnp.where(live, jnp.exp(s - peak), 0.0)
            out[y, 16 + h * 8 : 24 + h * 8, :] = columns([peak, jnp.sum(p, axis=1, keepdims=True)])
            probs.append(p)
        wide = []
        for b in range(8):
            for h in range(2):
                own = jnp.where(row == b, probs[h], 0.0)
                none = jnp.zeros((8, 128), F32)
                wide.append(jnp.concatenate([own, none] if h == 0 else [none, own], axis=0).astype(BF16))
        copies[y].wait()
        out[y, 0:16, :] = dot(jnp.concatenate(wide, axis=1), values[y * 8 : y * 8 + 8].reshape(2048, 128))


def merge_blocks(got, own, out):
    z = lax.axis_index("z")
    peaks = [got[k, 16:32, 0:1] for k in range(4)]
    totals = [got[k, 16:32, 1:2] for k in range(4)]
    mine = row_is(16, z)
    own_peak = jnp.where(mine, own[0:1, 0:1], masked_score)
    top = own_peak
    for peak in peaks:
        top = jnp.maximum(top, peak)
    own_weight = jnp.where(mine, jnp.exp(own_peak - top), 0.0)
    total = own_weight
    merged = own_weight * own[1:2, :]
    for k in range(4):
        weight = jnp.exp(peaks[k] - top)
        total = total + weight * totals[k]
        merged = merged + weight * got[k, 0:16]
    one = high(top)
    two = high(top - one)
    three = top - one - two
    four = high(total)
    five = total - four
    parts = []
    for h in range(2):
        for value in (one, two, three, four, five):
            parts.append(value[h * 8 : h * 8 + 8])
    extra = columns(parts).astype(BF16)
    merged = merged.astype(BF16)
    for k in range(16):
        out[k, 0:16, :] = merged
        out[k, 16:24, :] = extra


def project_out(got, w_all, gain_att, out):
    gain = gain_att[...].astype(F32)
    squares = jnp.zeros((8, 1), F32)
    part = jnp.zeros((8, 256), F32)
    extras = [got[k, 16:24, :].astype(F32) for k in range(16)]
    for h in range(2):
        c = h * 5
        peaks = [e[:, c : c + 1] + e[:, c + 1 : c + 2] + e[:, c + 2 : c + 3] for e in extras]
        top = peaks[0]
        for peak in peaks[1:]:
            top = jnp.maximum(top, peak)
        total = jnp.zeros((8, 1), F32)
        merged = jnp.zeros((8, 128), F32)
        for k in range(16):
            weight = jnp.exp(peaks[k] - top)
            total = total + weight * (extras[k][:, c + 3 : c + 4] + extras[k][:, c + 4 : c + 5])
            merged = merged + weight * got[k, 0:16, :].astype(F32)[h * 8 : h * 8 + 8]
        attended = merged / total
        squares = squares + jnp.sum(attended * attended, axis=1, keepdims=True)
        attended_in = (attended * gain[:, h * 128 : h * 128 + 128]).astype(BF16)
        w = jnp.concatenate([w_all[y, 16 + h * 64 : 80 + h * 64, :] for y in range(4)], axis=0)
        part = part + dot_nt(attended_in, w)
    extra = columns([squares])
    for k in range(8):
        out[k, 0:8, :] = part[:, 0:128]
        out[k, 8:16, :] = part[:, 128:256]
        out[k, 16:24, :] = extra


def mix_up(got, stream_all, gain_all, near, far, out, residual_out, halves):
    y = lax.axis_index("y")
    total = got[0]
    for k in range(1, 8):
        total = total + got[k]
    scale = lax.rsqrt(total[16:24, 0:1] / HEADS_WIDTH + norm_eps)
    squares = jnp.zeros((8, 1), F32)
    for k in range(2):
        residual = high(stream_all[k] + scale * total[k * 8 : k * 8 + 8])
        squares = squares + jnp.sum(residual * residual, axis=1, keepdims=True)
        mixer_in = high(residual * gain_all[k])
        halves[k] = mixer_in
        halves[2 + k] = pltpu.roll(mixer_in, 64, 1)
        residual_out[2 * k] = residual
        residual_out[2 * k + 1] = pltpu.roll(residual, 64, 1)
    up = dot(halves[y // 2 + 2 * (y % 2)].astype(BF16), near[...])
    up = up + dot(halves[1 - y // 2 + 2 * (1 - y % 2)].astype(BF16), far[...])
    one = high(squares)
    two = high(squares - one)
    extra = columns([one, two, squares - one - two])
    for k in range(16):
        both = jnp.concatenate([up[:, k * 128 : k * 128 + 128], extra], axis=0)
        out[k] = both.astype(BF16)


def activate(got, out):
    total = got[0].astype(F32)
    for k in range(1, 16):
        total = total + got[k].astype(F32)
    squares = total[8:16, 0:1] + total[8:16, 1:2] + total[8:16, 2:3]
    scale = lax.rsqrt(squares / WIDTH + norm_eps)
    hidden = jnp.square(jnp.maximum(total[0:8] * scale, 0.0)).astype(BF16)
    for k in range(16):
        out[k] = hidden


def mix_down(got, residual, near, far, out):
    y = lax.axis_index("y")
    t = lax.axis_index("tp")
    hidden = jnp.concatenate([got[k] for k in range(16)], axis=1)
    places = ((y, y + 1 - 2 * (y % 2)), (3 - y, (y + 2) % 4))
    for w, targets in zip((near, far), places):
        both = dot_nt(hidden, w[...])
        for target, part in zip(targets, (both, pltpu.roll(both, 64, 1))):
            part = part + jnp.where(t == 0, residual[target], 0.0)
            for k in range(8):
                out[target * 8 + k] = part


def finish(got, out):
    for y in range(4):
        total = got[y * 8]
        for k in range(1, 8):
            total = total + got[y * 8 + k]
        out[y * 8 : y * 8 + 8, :] = total[:, 0:64].astype(BF16)


def call(kernel, outs, *args, near=(0,), anywhere=(), scalars=(), scratch=()):
    specs = []
    placed = []
    for k, a in enumerate(args):
        space = pl.ANY if k in anywhere else pltpu.SMEM if k in scalars else pltpu.VMEM
        specs.append(pl.BlockSpec(memory_space=space))
        if k not in scalars:
            a = pltpu.with_memory_space_constraint(a, pltpu.VMEM if k in near else pltpu.HBM)
        placed.append(a)
    shapes = [pltpu.VMEM(s, d) for s, d in outs]
    found = pl.pallas_call(
        kernel,
        out_shape=shapes,
        in_specs=specs,
        out_specs=[pl.BlockSpec(memory_space=pltpu.VMEM) for _ in shapes],
        scratch_shapes=list(scratch),
        compiler_params=pltpu.CompilerParams(vmem_limit_bytes=LIMIT),
    )(*placed)
    return found if len(shapes) > 1 else found[0]


def fetch(keys, w_out, decay, keys_out, w_out_out, decay_out, sems):
    pairs = ((keys, keys_out), (w_out, w_out_out), (decay, decay_out))
    copies = [pltpu.make_async_copy(a, b, sems.at[k]) for k, (a, b) in enumerate(pairs)]
    for copy in copies:
        copy.start()
    for copy in copies:
        copy.wait()


def beside(value):
    return lax.ppermute(value, "y", [(0, 1), (1, 0), (2, 3), (3, 2)])


def across(value):
    return lax.ppermute(value, "y", [(0, 3), (3, 0), (1, 2), (2, 1)])


def layer(
    stream,
    gain_in,
    w_query,
    w_key,
    w_value,
    w_forget,
    keys_cache,
    values_cache,
    decay_cache,
    lengths,
    gain_att,
    w_out,
    gain_mlp,
    w_up,
    w_down,
):
    lines = call(
        project,
        [((4, 64, 128), F32)],
        stream,
        gain_in.reshape(1, 64),
        gain_mlp.reshape(1, 64),
        w_query,
        w_key,
        w_value,
        w_forget.T,
        near=(),
        anywhere=(6,),
        scratch=(pltpu.VMEM((16, 128), BF16), pltpu.SemaphoreType.DMA),
    )
    got = swap(lines, "y")
    lines, stream_all, gain_all = call(
        spread_rows, [((16, 32, 128), BF16), ((2, 8, 128), F32), ((2, 8, 128), F32)], got
    )
    lines, w_up, keys_cache = lax.optimization_barrier((lines, w_up, keys_cache))
    got = swap(lines, "z")
    keys, w_out, decay = call(
        fetch,
        [(keys_cache.shape, BF16), ((64, 256), BF16), (decay_cache.shape, F32)],
        keys_cache,
        w_out.T,
        decay_cache,
        near=(),
        anywhere=(0, 1, 2),
        scratch=(pltpu.SemaphoreType.DMA((3,)),),
    )
    other = beside(w_up)
    lines, own = call(finish_rows, [((4, 144, 128), BF16), ((8, 128), F32)], got, w_out, near=(0, 1))
    lines, other = lax.optimization_barrier((lines, other))
    w_all = swap(lines, "y")
    lines = call(
        attend,
        [((4, 32, 128), F32)],
        w_all,
        keys,
        values_cache,
        decay,
        lengths,
        near=(0, 1, 3),
        anywhere=(2,),
        scalars=(4,),
        scratch=(pltpu.VMEM((32, 2, 128, 128), BF16), pltpu.SemaphoreType.DMA((4,))),
    )
    got = swap(lines, "y")
    lines = call(merge_blocks, [((16, 24, 128), BF16)], got, own, near=(0, 1))
    up_near = jnp.concatenate([w_up, other], axis=0)
    lines, up_near, w_down = lax.optimization_barrier((lines, up_near, w_down.T))
    got = swap(lines, "z")
    up_far = across(up_near)
    other = beside(w_down)
    lines = call(project_out, [((8, 24, 128), F32)], got, w_all, gain_att.reshape(1, 256), near=(0, 1))
    got = swap(lines, "tp")
    lines, residual = call(
        mix_up,
        [((16, 16, 128), BF16), ((4, 8, 128), F32)],
        got,
        stream_all,
        gain_all,
        up_near,
        up_far,
        near=tuple(range(5)),
        scratch=(pltpu.VMEM((4, 8, 128), F32),),
    )
    down_near = jnp.concatenate([w_down, other], axis=0)
    lines, down_near = lax.optimization_barrier((lines, down_near))
    got = swap(lines, "z")
    down_far = across(down_near)
    got = swap(call(activate, [((16, 8, 128), BF16)], got), "z")
    lines = call(mix_down, [((32, 8, 128), F32)], got, residual, down_near, down_far, near=tuple(range(4)))
    got = swap(lines, ("y", "tp"))
    return call(finish, [((32, 64), BF16)], got)


def solution(mesh):
    split = Mesh(mesh.devices.reshape(16, 4, mesh.shape["tp"]), ("z", "y", "tp"))
    return jax.shard_map(
        layer,
        mesh=split,
        in_specs=(
            P(None, KV),
            P(KV),
            P(KV, "tp"),
            P(KV, "tp"),
            P(KV, "tp"),
            P(),
            P(None, "tp", KV, None),
            P(None, "tp", KV, None),
            P(None, "tp", KV),
            P(),
            P("tp"),
            P("tp", KV),
            P(KV),
            P(KV, "tp"),
            P("tp", KV),
        ),
        out_specs=P(None, KV),
        check_vma=False,
    )
```

```python
import math

import jax
import jax.numpy as jnp
from jax import lax
from jax.experimental import pallas as pl
from jax.experimental.pallas import tpu as pltpu
from jax.sharding import Mesh
from jax.sharding import PartitionSpec as P

KV = ("z", "y")
norm_eps = 1e-06
masked_score = -1e30
F32 = jnp.float32
BF16 = jnp.bfloat16
LIMIT = 8 * 1024 * 1024
WIDTH = 4096
HEADS_WIDTH = 2048


def swap(value, axis):
    return lax.all_to_all(value, axis, split_axis=0, concat_axis=0, tiled=True)


def dot(a, b):
    return jnp.dot(a, b, preferred_element_type=F32)


def dot_nt(a, b):
    return lax.dot_general(a, b, (((1,), (1,)), ((), ())), preferred_element_type=F32)


def lanes(rows):
    return lax.broadcasted_iota(jnp.int32, (rows, 128), 1)


def row_is(count, index):
    return lax.broadcasted_iota(jnp.int32, (count, 1), 0) == index


def high(value):
    return value.astype(BF16).astype(F32)


def columns(values):
    lane = lanes(values[0].shape[0])
    tile = jnp.zeros(lane.shape, F32)
    for k, value in enumerate(values):
        tile = jnp.where(lane == k, value, tile)
    return tile


def project(stream, gain_in, gain_mlp, w_query, w_key, w_value, w_forget, out, gate_rows, sem):
    kv = lax.axis_index("z") * 4 + lax.axis_index("y")
    head = lax.axis_index("tp") * 2
    start = pl.multiple_of((kv // 2) * 128, 128)
    copy = pltpu.make_async_copy(w_forget.at[:, pl.ds(start, 128)], gate_rows, sem)
    copy.start()
    x = stream[...].astype(F32)
    scaled = (x * gain_in[...].astype(F32)).astype(BF16)
    squares = jnp.sum(x * x, axis=1, keepdims=True)
    for k, w in enumerate((w_query, w_key, w_value)):
        part = dot(scaled, w[...])
        for y in range(4):
            for h in range(2):
                out[y, k * 16 + h * 8 : k * 16 + h * 8 + 8, :] = part[y * 8 : y * 8 + 8, h * 128 : h * 128 + 128]
    copy.wait()
    wide = jnp.concatenate([scaled, scaled], axis=1)
    wide = jnp.where(lanes(32) // 64 == kv % 2, wide.astype(F32), 0.0).astype(BF16)
    gates = dot_nt(wide, gate_rows[...])
    column = lax.broadcasted_iota(jnp.int32, gates.shape, 1)
    first = jnp.sum(jnp.where(column == head, gates, 0.0), axis=1, keepdims=True)
    second = jnp.sum(jnp.where(column == head + 1, gates, 0.0), axis=1, keepdims=True)
    gain = gain_mlp[...].astype(F32)
    gain = jnp.broadcast_to(jnp.concatenate([gain, gain], axis=1), (32, 128))
    extra = jnp.where(lanes(32) < 64, columns([squares, first, second]), gain)
    twice = jnp.concatenate([x, x], axis=1)
    for y in range(4):
        out[y, 48:56, :] = extra[y * 8 : y * 8 + 8]
        out[y, 56:64, :] = twice[y * 8 : y * 8 + 8]


def spread_rows(got, out, stream_all, gain_all):
    total = got[0, 0:56] + got[1, 0:56] + got[2, 0:56] + got[3, 0:56]
    q = total[0:16].astype(BF16)
    x = jnp.where(lanes(8) < 3, total[48:56], 0.0)
    one = high(x)
    both = one + pltpu.roll(high(x - one), 3, 1)
    both = jnp.transpose(jnp.concatenate([both, jnp.zeros((120, 128), F32)], axis=0))[0:8]
    row = lax.broadcasted_iota(jnp.int32, (8, 128), 0)
    for p in range(16):
        k = total[16 + p : 17 + p]
        v = total[32 + p : 33 + p]
        out[p, 0:16, :] = q
        out[p, 16:24, :] = jnp.where(row == 6, k, jnp.where(row == 7, v, both)).astype(BF16)
    left = lanes(8) < 64
    for k in range(2):
        stream_all[k] = jnp.where(left, got[2 * k, 56:64], got[2 * k + 1, 56:64])
        gain_all[k] = jnp.where(left, pltpu.roll(got[2 * k, 48:56], 64, 1), got[2 * k + 1, 48:56])


def finish_rows(got, w_out, out, own_out):
    z = lax.axis_index("z")
    total = got[0].astype(F32)
    for k in range(1, 16):
        total = total + got[k].astype(F32)
    x = jnp.concatenate([total[16:24], jnp.zeros((120, 128), F32)], axis=0)
    x = jnp.transpose(x)[0:8]
    x = x + pltpu.roll(x, 125, 1)
    scale = lax.rsqrt(x[:, 0:1] / WIDTH + norm_eps)
    scale = jnp.concatenate([scale, scale], axis=0)
    gate = jnp.concatenate([x[:, 1:2], x[:, 2:3]], axis=0) * scale
    q = (total[0:16] * scale).astype(BF16)
    mine = row_is(16, z)
    scale_z = jnp.sum(jnp.where(mine, scale, 0.0), axis=0, keepdims=True)
    gate_z = jnp.sum(jnp.where(mine, gate, 0.0), axis=0, keepdims=True)
    k = high(total[22:23] * scale_z)
    v = high(total[23:24] * scale_z)
    q_z = jnp.sum(jnp.where(mine, q.astype(F32), 0.0), axis=0, keepdims=True)
    own = jnp.sum(q_z * k, axis=1, keepdims=True) * (1.0 / math.sqrt(128))
    own = own + jnp.maximum(-gate_z, 0.0) + jnp.log1p(jnp.exp(-jnp.abs(gate_z)))
    row = lax.broadcasted_iota(jnp.int32, (8, 128), 0)
    own_out[...] = jnp.where(row == 0, own, v)
    w = w_out[...]
    for y in range(4):
        out[y, 0:16, :] = q
        out[y, 16:80, :] = w[:, 0:128]
        out[y, 80:144, :] = w[:, 128:256]


def attend(w_all, keys, values_far, decay, lengths, out, values, sems):
    copies = []
    for y in range(4):
        part = pl.ds(y * 8, 8)
        copies.append(pltpu.make_async_copy(values_far.at[part], values.at[part], sems.at[y]))
        copies[y].start()
    first = (lax.axis_index("z") * 4 + lax.axis_index("y")) * 128
    place = lanes(8) + first
    row = lax.broadcasted_iota(jnp.int32, (8, 128), 0)
    for y in range(4):
        q = w_all[y, 0:16, :]
        every = dot_nt(q, keys[y * 8 : y * 8 + 8].reshape(2048, 128))
        length = jnp.zeros((8, 128), jnp.int32)
        for b in range(8):
            length = jnp.where(row == b, lengths[y * 8 + b], length)
        live = place < length
        probs = []
        for h in range(2):
            s = jnp.zeros((8, 128), F32)
            for b in range(8):
                c = (b * 2 + h) * 128
                s = jnp.where(row == b, every[h * 8 : h * 8 + 8, c : c + 128], s)
            s = s * (1.0 / math.sqrt(128)) + decay[y * 8 : y * 8 + 8, h, :]
            s = jnp.where(live, s, masked_score)
            peak = jnp.max(s, axis=1, keepdims=True)
            p = jnp.where(live, jnp.exp(s - peak), 0.0)
            out[y, 16 + h * 8 : 24 + h * 8, :] = columns([peak, jnp.sum(p, axis=1, keepdims=True)])
            probs.append(p)
        wide = []
        for b in range(8):
            for h in range(2):
                own = jnp.where(row == b, probs[h], 0.0)
                none = jnp.zeros((8, 128), F32)
                wide.append(jnp.concatenate([own, none] if h == 0 else [none, own], axis=0).astype(BF16))
        copies[y].wait()
        out[y, 0:16, :] = dot(jnp.concatenate(wide, axis=1), values[y * 8 : y * 8 + 8].reshape(2048, 128))


def merge_blocks(got, own, out):
    z = lax.axis_index("z")
    peaks = [got[k, 16:32, 0:1] for k in range(4)]
    totals = [got[k, 16:32, 1:2] for k in range(4)]
    mine = row_is(16, z)
    own_peak = jnp.where(mine, own[0:1, 0:1], masked_score)
    top = own_peak
    for peak in peaks:
        top = jnp.maximum(top, peak)
    own_weight = jnp.where(mine, jnp.exp(own_peak - top), 0.0)
    total = own_weight
    merged = own_weight * own[1:2, :]
    for k in range(4):
        weight = jnp.exp(peaks[k] - top)
        total = total + weight * totals[k]
        merged = merged + weight * got[k, 0:16]
    one = high(top)
    two = high(top - one)
    three = top - one - two
    four = high(total)
    five = total - four
    parts = []
    for h in range(2):
        for value in (one, two, three, four, five):
            parts.append(value[h * 8 : h * 8 + 8])
    extra = columns(parts).astype(BF16)
    merged = merged.astype(BF16)
    for k in range(16):
        out[k, 0:16, :] = merged
        out[k, 16:24, :] = extra


def project_out(got, w_all, gain_att, out):
    gain = gain_att[...].astype(F32)
    squares = jnp.zeros((8, 1), F32)
    part = jnp.zeros((8, 256), F32)
    extras = [got[k, 16:24, :].astype(F32) for k in range(16)]
    for h in range(2):
        c = h * 5
        peaks = [e[:, c : c + 1] + e[:, c + 1 : c + 2] + e[:, c + 2 : c + 3] for e in extras]
        top = peaks[0]
        for peak in peaks[1:]:
            top = jnp.maximum(top, peak)
        total = jnp.zeros((8, 1), F32)
        merged = jnp.zeros((8, 128), F32)
        for k in range(16):
            weight = jnp.exp(peaks[k] - top)
            total = total + weight * (extras[k][:, c + 3 : c + 4] + extras[k][:, c + 4 : c + 5])
            merged = merged + weight * got[k, 0:16, :].astype(F32)[h * 8 : h * 8 + 8]
        attended = merged / total
        squares = squares + jnp.sum(attended * attended, axis=1, keepdims=True)
        attended_in = (attended * gain[h : h + 1]).astype(BF16)
        w = jnp.concatenate([w_all[y, 16 + h * 64 : 80 + h * 64, :] for y in range(4)], axis=0)
        part = part + dot_nt(attended_in, w)
    extra = columns([squares])
    for k in range(8):
        out[k, 0:8, :] = part[:, 0:128]
        out[k, 8:16, :] = part[:, 128:256]
        out[k, 16:24, :] = extra


def mix_up(got, stream_all, gain_all, near, far, out, residual_out, halves):
    y = lax.axis_index("y")
    total = got[0]
    for k in range(1, 8):
        total = total + got[k]
    scale = lax.rsqrt(total[16:24, 0:1] / HEADS_WIDTH + norm_eps)
    squares = jnp.zeros((8, 1), F32)
    for k in range(2):
        residual = high(stream_all[k] + scale * total[k * 8 : k * 8 + 8])
        squares = squares + jnp.sum(residual * residual, axis=1, keepdims=True)
        mixer_in = high(residual * gain_all[k])
        halves[k] = mixer_in
        halves[2 + k] = pltpu.roll(mixer_in, 64, 1)
        residual_out[2 * k] = residual
        residual_out[2 * k + 1] = pltpu.roll(residual, 64, 1)
    up = dot(halves[y // 2 + 2 * (y % 2)].astype(BF16), near[0:128, :])
    up = up + dot(halves[1 - y // 2 + 2 * (1 - y % 2)].astype(BF16), far[0:128, :])
    one = high(squares)
    two = high(squares - one)
    extra = columns([one, two, squares - one - two])
    for k in range(16):
        both = jnp.concatenate([up[:, k * 128 : k * 128 + 128], extra], axis=0)
        out[k] = both.astype(BF16)


def activate(got, out):
    total = got[0].astype(F32)
    for k in range(1, 16):
        total = total + got[k].astype(F32)
    squares = total[8:16, 0:1] + total[8:16, 1:2] + total[8:16, 2:3]
    scale = lax.rsqrt(squares / WIDTH + norm_eps)
    hidden = jnp.square(jnp.maximum(total[0:8] * scale, 0.0)).astype(BF16)
    for k in range(16):
        out[k] = hidden


def mix_down(got, residual, near, far, out):
    y = lax.axis_index("y")
    t = lax.axis_index("tp")
    hidden = jnp.concatenate([got[k] for k in range(16)], axis=1)
    places = ((y, y + 1 - 2 * (y % 2)), (3 - y, (y + 2) % 4))
    for w, targets in zip((near, far), places):
        both = dot_nt(hidden, w[...])
        for target, part in zip(targets, (both, pltpu.roll(both, 64, 1))):
            part = part + jnp.where(t == 0, residual[target], 0.0)
            for k in range(8):
                out[target * 8 + k] = part


def finish(got, out):
    for y in range(4):
        total = got[y * 8]
        for k in range(1, 8):
            total = total + got[y * 8 + k]
        out[y * 8 : y * 8 + 8, :] = total[:, 0:64].astype(BF16)


def call(kernel, outs, *args, near=(0,), anywhere=(), scalars=(), scratch=()):
    specs = []
    placed = []
    for k, a in enumerate(args):
        space = pl.ANY if k in anywhere else pltpu.SMEM if k in scalars else pltpu.VMEM
        specs.append(pl.BlockSpec(memory_space=space))
        if k not in scalars:
            a = pltpu.with_memory_space_constraint(a, pltpu.VMEM if k in near else pltpu.HBM)
        placed.append(a)
    shapes = [pltpu.VMEM(s, d) for s, d in outs]
    found = pl.pallas_call(
        kernel,
        out_shape=shapes,
        in_specs=specs,
        out_specs=[pl.BlockSpec(memory_space=pltpu.VMEM) for _ in shapes],
        scratch_shapes=list(scratch),
        compiler_params=pltpu.CompilerParams(vmem_limit_bytes=LIMIT),
    )(*placed)
    return found if len(shapes) > 1 else found[0]


def fetch(keys, w_out, decay, gain, keys_out, w_out_out, decay_out, gain_out, sems):
    pairs = ((keys, keys_out), (w_out, w_out_out), (decay, decay_out), (gain, gain_out))
    copies = [pltpu.make_async_copy(a, b, sems.at[k]) for k, (a, b) in enumerate(pairs)]
    for copy in copies:
        copy.start()
    for copy in copies:
        copy.wait()


def beside(value):
    return lax.ppermute(value, "y", [(0, 1), (1, 0), (2, 3), (3, 2)])


def across(value):
    return lax.ppermute(value, "y", [(0, 3), (3, 0), (1, 2), (2, 1)])


def layer(
    stream,
    gain_in,
    w_query,
    w_key,
    w_value,
    w_forget,
    keys_cache,
    values_cache,
    decay_cache,
    lengths,
    gain_att,
    w_out,
    gain_mlp,
    w_up,
    w_down,
):
    lines = call(
        project,
        [((4, 64, 128), F32)],
        stream,
        gain_in.reshape(1, 64),
        gain_mlp.reshape(1, 64),
        w_query,
        w_key,
        w_value,
        w_forget.T,
        near=(),
        anywhere=(6,),
        scratch=(pltpu.VMEM((16, 128), BF16), pltpu.SemaphoreType.DMA),
    )
    got = swap(lines, "y")
    lines, stream_all, gain_all = call(
        spread_rows, [((16, 24, 128), BF16), ((2, 8, 128), F32), ((2, 8, 128), F32)], got
    )
    lines, keys_cache = lax.optimization_barrier((lines, keys_cache))
    got = swap(lines, "z")
    keys, w_out, decay, gain_att = call(
        fetch,
        [(keys_cache.shape, BF16), ((64, 256), BF16), (decay_cache.shape, F32), ((2, 128), BF16)],
        keys_cache,
        w_out.T,
        decay_cache,
        gain_att.reshape(2, 128),
        near=(),
        anywhere=(0, 1, 2, 3),
        scratch=(pltpu.SemaphoreType.DMA((4,)),),
    )
    other = beside(w_up)
    lines, own = call(finish_rows, [((4, 144, 128), BF16), ((8, 128), F32)], got, w_out, near=(0, 1))
    lines, other = lax.optimization_barrier((lines, other))
    up_near = jnp.concatenate([w_up, other], axis=0)
    w_all = swap(lines, "y")
    lines = call(
        attend,
        [((4, 32, 128), F32)],
        w_all,
        keys,
        values_cache,
        decay,
        lengths,
        near=(0, 1, 3),
        anywhere=(2,),
        scalars=(4,),
        scratch=(pltpu.VMEM((32, 2, 128, 128), BF16), pltpu.SemaphoreType.DMA((4,))),
    )
    lines, up_near = lax.optimization_barrier((lines, up_near))
    got = swap(lines, "y")
    up_far = across(up_near)
    lines = call(merge_blocks, [((16, 24, 128), BF16)], got, own, near=(0, 1))
    lines, w_down = lax.optimization_barrier((lines, w_down.T))
    got = swap(lines, "z")
    other = beside(w_down)
    lines = call(project_out, [((8, 24, 128), F32)], got, w_all, gain_att, near=(0, 1, 2))
    got = swap(lines, "tp")
    lines, residual = call(
        mix_up,
        [((16, 16, 128), BF16), ((4, 8, 128), F32)],
        got,
        stream_all,
        gain_all,
        up_near,
        up_far,
        near=tuple(range(5)),
        scratch=(pltpu.VMEM((4, 8, 128), F32),),
    )
    down_near = jnp.concatenate([w_down, other], axis=0)
    lines, down_near = lax.optimization_barrier((lines, down_near))
    got = swap(lines, "z")
    down_far = across(down_near)
    got = swap(call(activate, [((16, 8, 128), BF16)], got), "z")
    lines = call(mix_down, [((32, 8, 128), F32)], got, residual, down_near, down_far, near=tuple(range(4)))
    got = swap(lines, ("y", "tp"))
    return call(finish, [((32, 64), BF16)], got)


def solution(mesh):
    split = Mesh(mesh.devices.reshape(16, 4, mesh.shape["tp"]), ("z", "y", "tp"))
    return jax.shard_map(
        layer,
        mesh=split,
        in_specs=(
            P(None, KV),
            P(KV),
            P(KV, "tp"),
            P(KV, "tp"),
            P(KV, "tp"),
            P(),
            P(None, "tp", KV, None),
            P(None, "tp", KV, None),
            P(None, "tp", KV),
            P(),
            P("tp"),
            P("tp", KV),
            P(KV),
            P(KV, "tp"),
            P("tp", KV),
        ),
        out_specs=P(None, KV),
        check_vma=False,
    )
```

```python
import math

import jax
import jax.numpy as jnp
from jax import lax
from jax.experimental import pallas as pl
from jax.experimental.pallas import tpu as pltpu
from jax.sharding import Mesh
from jax.sharding import PartitionSpec as P

KV = ("z", "y")
norm_eps = 1e-06
masked_score = -1e30
F32 = jnp.float32
BF16 = jnp.bfloat16
LIMIT = 8 * 1024 * 1024
WIDTH = 4096
HEADS_WIDTH = 2048


def swap(value, axis):
    return lax.all_to_all(value, axis, split_axis=0, concat_axis=0, tiled=True)


def dot(a, b):
    return jnp.dot(a, b, preferred_element_type=F32)


def dot_nt(a, b):
    return lax.dot_general(a, b, (((1,), (1,)), ((), ())), preferred_element_type=F32)


def lanes(rows):
    return lax.broadcasted_iota(jnp.int32, (rows, 128), 1)


def row_is(count, index):
    return lax.broadcasted_iota(jnp.int32, (count, 1), 0) == index


def high(value):
    return value.astype(BF16).astype(F32)


def columns(values):
    lane = lanes(values[0].shape[0])
    tile = jnp.zeros(lane.shape, F32)
    for k, value in enumerate(values):
        tile = jnp.where(lane == k, value, tile)
    return tile


def project(stream, gain_in, gain_mlp, w_query, w_key, w_value, w_forget, out, gate_rows, sem):
    kv = lax.axis_index("z") * 4 + lax.axis_index("y")
    head = lax.axis_index("tp") * 2
    start = pl.multiple_of((kv // 2) * 128, 128)
    copy = pltpu.make_async_copy(w_forget.at[:, pl.ds(start, 128)], gate_rows, sem)
    copy.start()
    x = stream[...].astype(F32)
    scaled = (x * gain_in[...].astype(F32)).astype(BF16)
    squares = jnp.sum(x * x, axis=1, keepdims=True)
    for k, w in enumerate((w_query, w_key, w_value)):
        part = dot(scaled, w[...])
        for y in range(4):
            for h in range(2):
                out[y, k * 16 + h * 8 : k * 16 + h * 8 + 8, :] = part[y * 8 : y * 8 + 8, h * 128 : h * 128 + 128]
    copy.wait()
    wide = jnp.concatenate([scaled, scaled], axis=1)
    wide = jnp.where(lanes(32) // 64 == kv % 2, wide.astype(F32), 0.0).astype(BF16)
    gates = dot_nt(wide, gate_rows[...])
    column = lax.broadcasted_iota(jnp.int32, gates.shape, 1)
    first = jnp.sum(jnp.where(column == head, gates, 0.0), axis=1, keepdims=True)
    second = jnp.sum(jnp.where(column == head + 1, gates, 0.0), axis=1, keepdims=True)
    gain = gain_mlp[...].astype(F32)
    gain = jnp.broadcast_to(jnp.concatenate([gain, gain], axis=1), (32, 128))
    extra = jnp.where(lanes(32) < 64, columns([squares, first, second]), gain)
    twice = jnp.concatenate([x, x], axis=1)
    for y in range(4):
        out[y, 48:56, :] = extra[y * 8 : y * 8 + 8]
        out[y, 56:64, :] = twice[y * 8 : y * 8 + 8]


def spread_rows(got, out, stream_all, gain_all):
    total = got[0, 0:56] + got[1, 0:56] + got[2, 0:56] + got[3, 0:56]
    q = total[0:16].astype(BF16)
    x = jnp.where(lanes(8) < 3, total[48:56], 0.0)
    one = high(x)
    both = one + pltpu.roll(high(x - one), 3, 1)
    both = jnp.transpose(jnp.concatenate([both, jnp.zeros((120, 128), F32)], axis=0))[0:8]
    row = lax.broadcasted_iota(jnp.int32, (8, 128), 0)
    for p in range(16):
        k = total[16 + p : 17 + p]
        v = total[32 + p : 33 + p]
        out[p, 0:16, :] = q
        out[p, 16:24, :] = jnp.where(row == 6, k, jnp.where(row == 7, v, both)).astype(BF16)
    left = lanes(8) < 64
    for k in range(2):
        stream_all[k] = jnp.where(left, got[2 * k, 56:64], got[2 * k + 1, 56:64])
        gain_all[k] = jnp.where(left, pltpu.roll(got[2 * k, 48:56], 64, 1), got[2 * k + 1, 48:56])


def finish_rows(got, w_out, out, own_out):
    z = lax.axis_index("z")
    total = got[0].astype(F32)
    for k in range(1, 16):
        total = total + got[k].astype(F32)
    x = jnp.concatenate([total[16:24], jnp.zeros((120, 128), F32)], axis=0)
    x = jnp.transpose(x)[0:8]
    x = x + pltpu.roll(x, 125, 1)
    scale = lax.rsqrt(x[:, 0:1] / WIDTH + norm_eps)
    scale = jnp.concatenate([scale, scale], axis=0)
    gate = jnp.concatenate([x[:, 1:2], x[:, 2:3]], axis=0) * scale
    q = (total[0:16] * scale).astype(BF16)
    mine = row_is(16, z)
    scale_z = jnp.sum(jnp.where(mine, scale, 0.0), axis=0, keepdims=True)
    gate_z = jnp.sum(jnp.where(mine, gate, 0.0), axis=0, keepdims=True)
    k = high(total[22:23] * scale_z)
    v = high(total[23:24] * scale_z)
    q_z = jnp.sum(jnp.where(mine, q.astype(F32), 0.0), axis=0, keepdims=True)
    own = jnp.sum(q_z * k, axis=1, keepdims=True) * (1.0 / math.sqrt(128))
    own = own + jnp.maximum(-gate_z, 0.0) + jnp.log1p(jnp.exp(-jnp.abs(gate_z)))
    row = lax.broadcasted_iota(jnp.int32, (8, 128), 0)
    own_out[...] = jnp.where(row == 0, own, v)
    w = w_out[...]
    for y in range(4):
        out[y, 0:16, :] = q
        out[y, 16:80, :] = w[:, 0:128]
        out[y, 80:144, :] = w[:, 128:256]


def attend(w_all, keys, values_far, decay, lengths, out, values, sems):
    copies = []
    for y in range(4):
        part = pl.ds(y * 8, 8)
        copies.append(pltpu.make_async_copy(values_far.at[part], values.at[part], sems.at[y]))
        copies[y].start()
    first = (lax.axis_index("z") * 4 + lax.axis_index("y")) * 128
    place = lanes(8) + first
    row = lax.broadcasted_iota(jnp.int32, (8, 128), 0)
    for y in range(4):
        q = w_all[y, 0:16, :]
        every = dot_nt(q, keys[y * 8 : y * 8 + 8].reshape(2048, 128))
        live = place < lengths[y]
        probs = []
        for h in range(2):
            s = jnp.zeros((8, 128), F32)
            for b in range(8):
                c = (b * 2 + h) * 128
                s = jnp.where(row == b, every[h * 8 : h * 8 + 8, c : c + 128], s)
            s = s * (1.0 / math.sqrt(128)) + decay[y * 8 : y * 8 + 8, h, :]
            s = jnp.where(live, s, masked_score)
            peak = jnp.max(s, axis=1, keepdims=True)
            p = jnp.where(live, jnp.exp(s - peak), 0.0)
            out[y, 16 + h * 8 : 24 + h * 8, :] = columns([peak, jnp.sum(p, axis=1, keepdims=True)])
            probs.append(p)
        wide = []
        for b in range(8):
            for h in range(2):
                own = jnp.where(row == b, probs[h], 0.0)
                none = jnp.zeros((8, 128), F32)
                wide.append(jnp.concatenate([own, none] if h == 0 else [none, own], axis=0).astype(BF16))
        copies[y].wait()
        found = values[y * 8 : y * 8 + 8].reshape(2048, 128)
        out[y, 0:16, :] = dot(jnp.concatenate(wide, axis=1), found)


def merge_blocks(got, own, out):
    z = lax.axis_index("z")
    peaks = [got[k, 16:32, 0:1] for k in range(4)]
    totals = [got[k, 16:32, 1:2] for k in range(4)]
    mine = row_is(16, z)
    own_peak = jnp.where(mine, own[0:1, 0:1], masked_score)
    top = own_peak
    for peak in peaks:
        top = jnp.maximum(top, peak)
    own_weight = jnp.where(mine, jnp.exp(own_peak - top), 0.0)
    total = own_weight
    merged = own_weight * own[1:2, :]
    for k in range(4):
        weight = jnp.exp(peaks[k] - top)
        total = total + weight * totals[k]
        merged = merged + weight * got[k, 0:16]
    one = high(top)
    two = high(top - one)
    three = top - one - two
    four = high(total)
    five = total - four
    parts = []
    for h in range(2):
        for value in (one, two, three, four, five):
            parts.append(value[h * 8 : h * 8 + 8])
    extra = columns(parts).astype(BF16)
    merged = merged.astype(BF16)
    for k in range(16):
        out[k, 0:16, :] = merged
        out[k, 16:24, :] = extra


def project_out(got, w_all, gain_att, out):
    gain = gain_att[...].astype(F32)
    squares = jnp.zeros((8, 1), F32)
    part = jnp.zeros((8, 256), F32)
    extras = [got[k, 16:24, :].astype(F32) for k in range(16)]
    for h in range(2):
        c = h * 5
        peaks = [e[:, c : c + 1] + e[:, c + 1 : c + 2] + e[:, c + 2 : c + 3] for e in extras]
        top = peaks[0]
        for peak in peaks[1:]:
            top = jnp.maximum(top, peak)
        total = jnp.zeros((8, 1), F32)
        merged = jnp.zeros((8, 128), F32)
        for k in range(16):
            weight = jnp.exp(peaks[k] - top)
            total = total + weight * (extras[k][:, c + 3 : c + 4] + extras[k][:, c + 4 : c + 5])
            merged = merged + weight * got[k, 0:16, :].astype(F32)[h * 8 : h * 8 + 8]
        attended = merged / total
        squares = squares + jnp.sum(attended * attended, axis=1, keepdims=True)
        attended_in = (attended * gain[h : h + 1]).astype(BF16)
        w = jnp.concatenate([w_all[y, 16 + h * 64 : 80 + h * 64, :] for y in range(4)], axis=0)
        part = part + dot_nt(attended_in, w)
    extra = columns([squares])
    for k in range(8):
        out[k, 0:8, :] = part[:, 0:128]
        out[k, 8:16, :] = part[:, 128:256]
        out[k, 16:24, :] = extra


def mix_up(got, stream_all, gain_all, near, far, w_down, other, out, residual_out, down_near, halves):
    down_near[0:64, :] = w_down[...]
    down_near[64:128, :] = other[...]
    y = lax.axis_index("y")
    total = got[0]
    for k in range(1, 8):
        total = total + got[k]
    scale = lax.rsqrt(total[16:24, 0:1] / HEADS_WIDTH + norm_eps)
    squares = jnp.zeros((8, 1), F32)
    for k in range(2):
        residual = high(stream_all[k] + scale * total[k * 8 : k * 8 + 8])
        squares = squares + jnp.sum(residual * residual, axis=1, keepdims=True)
        mixer_in = high(residual * gain_all[k])
        halves[k] = mixer_in
        halves[2 + k] = pltpu.roll(mixer_in, 64, 1)
        residual_out[2 * k] = residual
        residual_out[2 * k + 1] = pltpu.roll(residual, 64, 1)
    up = dot(halves[y // 2 + 2 * (y % 2)].astype(BF16), near[0:128, :])
    up = up + dot(halves[1 - y // 2 + 2 * (1 - y % 2)].astype(BF16), far[0:128, :])
    one = high(squares)
    two = high(squares - one)
    extra = columns([one, two, squares - one - two])
    for k in range(16):
        both = jnp.concatenate([up[:, k * 128 : k * 128 + 128], extra], axis=0)
        out[k] = both.astype(BF16)


def activate(got, out):
    total = got[0].astype(F32)
    for k in range(1, 16):
        total = total + got[k].astype(F32)
    squares = total[8:16, 0:1] + total[8:16, 1:2] + total[8:16, 2:3]
    scale = lax.rsqrt(squares / WIDTH + norm_eps)
    hidden = jnp.square(jnp.maximum(total[0:8] * scale, 0.0)).astype(BF16)
    for k in range(16):
        out[k] = hidden


def mix_down(got, residual, near, far, out):
    y = lax.axis_index("y")
    t = lax.axis_index("tp")
    hidden = jnp.concatenate([got[k] for k in range(16)], axis=1)
    places = ((y, y + 1 - 2 * (y % 2)), (3 - y, (y + 2) % 4))
    for w, targets in zip((near, far), places):
        both = dot_nt(hidden, w[...])
        for target, part in zip(targets, (both, pltpu.roll(both, 64, 1))):
            part = part + jnp.where(t == 0, residual[target], 0.0)
            for k in range(8):
                out[target * 8 + k] = part


def finish(got, out):
    for y in range(4):
        total = got[y * 8]
        for k in range(1, 8):
            total = total + got[y * 8 + k]
        out[y * 8 : y * 8 + 8, :] = total[:, 0:64].astype(BF16)


def call(kernel, outs, *args, near=(0,), anywhere=(), scalars=(), scratch=(), place=pltpu.VMEM):
    specs = []
    placed = []
    for k, a in enumerate(args):
        space = pl.ANY if k in anywhere else pltpu.SMEM if k in scalars else pltpu.VMEM
        specs.append(pl.BlockSpec(memory_space=space))
        if k not in scalars:
            a = pltpu.with_memory_space_constraint(a, pltpu.VMEM if k in near else pltpu.HBM)
        placed.append(a)
    shapes = [place(s, d) for s, d in outs]
    found = pl.pallas_call(
        kernel,
        out_shape=shapes,
        in_specs=specs,
        out_specs=[pl.BlockSpec(memory_space=pltpu.VMEM) for _ in shapes],
        scratch_shapes=list(scratch),
        compiler_params=pltpu.CompilerParams(vmem_limit_bytes=LIMIT),
    )(*placed)
    return found if len(shapes) > 1 else found[0]


def fetch(
    keys, w_out, decay, gain, w_up, other, lengths,
    keys_out, w_out_out, decay_out, gain_out, near, lengths_out, sems,
):
    pairs = (
        (keys, keys_out),
        (w_out, w_out_out),
        (decay, decay_out),
        (gain, gain_out),
        (w_up, near.at[0:64]),
    )
    copies = [pltpu.make_async_copy(a, b, sems.at[k]) for k, (a, b) in enumerate(pairs)]
    for copy in copies:
        copy.start()
    near[64:128, :] = other[...]
    row = lax.broadcasted_iota(jnp.int32, (8, 128), 0)
    for y in range(4):
        length = jnp.zeros((8, 128), jnp.int32)
        for b in range(8):
            length = jnp.where(row == b, lengths[y * 8 + b], length)
        lengths_out[y] = length
    for copy in copies:
        copy.wait()


def beside(value):
    return lax.ppermute(value, "y", [(0, 1), (1, 0), (2, 3), (3, 2)])


def across(value):
    return lax.ppermute(value, "y", [(0, 3), (3, 0), (1, 2), (2, 1)])


def layer(
    stream,
    gain_in,
    w_query,
    w_key,
    w_value,
    w_forget,
    keys_cache,
    values_cache,
    decay_cache,
    lengths,
    gain_att,
    w_out,
    gain_mlp,
    w_up,
    w_down,
):
    lines = call(
        project,
        [((4, 64, 128), F32)],
        stream,
        gain_in.reshape(1, 64),
        gain_mlp.reshape(1, 64),
        w_query,
        w_key,
        w_value,
        w_forget.T,
        near=(),
        anywhere=(6,),
        scratch=(pltpu.VMEM((16, 128), BF16), pltpu.SemaphoreType.DMA),
    )
    got = swap(lines, "y")
    lines, stream_all, gain_all = call(
        spread_rows, [((16, 24, 128), BF16), ((2, 8, 128), F32), ((2, 8, 128), F32)], got
    )
    lines, keys_cache = lax.optimization_barrier((lines, keys_cache))
    got = swap(lines, "z")
    other = beside(w_up)
    keys, w_out, decay, gain_att, up_near, lengths = call(
        fetch,
        [
            (keys_cache.shape, BF16),
            ((64, 256), BF16),
            (decay_cache.shape, F32),
            ((2, 128), BF16),
            ((128, 2048), BF16),
            ((4, 8, 128), jnp.int32),
        ],
        keys_cache,
        w_out.T,
        decay_cache,
        gain_att.reshape(2, 128),
        w_up,
        other,
        lengths,
        near=(5,),
        anywhere=(0, 1, 2, 3, 4),
        scalars=(6,),
        scratch=(pltpu.SemaphoreType.DMA((5,)),),
    )
    lines, own = call(finish_rows, [((4, 144, 128), BF16), ((8, 128), F32)], got, w_out, near=(0, 1))
    w_all = swap(lines, "y")
    lines = call(
        attend,
        [((4, 32, 128), F32)],
        w_all,
        keys,
        values_cache,
        decay,
        lengths,
        near=(0, 1, 3, 4),
        anywhere=(2,),
        scratch=(pltpu.VMEM((32, 2, 128, 128), BF16), pltpu.SemaphoreType.DMA((4,))),
    )
    lines, up_near = lax.optimization_barrier((lines, up_near))
    got = swap(lines, "y")
    up_far = across(up_near)
    lines = call(merge_blocks, [((16, 24, 128), BF16)], got, own, near=(0, 1))
    lines, w_down = lax.optimization_barrier((lines, w_down.T))
    got = swap(lines, "z")
    other = beside(w_down)
    lines = call(project_out, [((8, 24, 128), F32)], got, w_all, gain_att, near=(0, 1, 2))
    got = swap(lines, "tp")
    lines, residual, down_near = call(
        mix_up,
        [((16, 16, 128), BF16), ((4, 8, 128), F32), ((128, 2048), BF16)],
        got,
        stream_all,
        gain_all,
        up_near,
        up_far,
        w_down,
        other,
        near=tuple(range(7)),
        scratch=(pltpu.VMEM((4, 8, 128), F32),),
    )
    got = swap(lines, "z")
    down_far = across(down_near)
    got = swap(call(activate, [((16, 8, 128), BF16)], got), "z")
    lines = call(mix_down, [((32, 8, 128), F32)], got, residual, down_near, down_far, near=tuple(range(4)))
    got = swap(lines, ("y", "tp"))
    return call(finish, [((32, 64), BF16)], got, place=pltpu.HBM)


def solution(mesh):
    split = Mesh(mesh.devices.reshape(16, 4, mesh.shape["tp"]), ("z", "y", "tp"))
    return jax.shard_map(
        layer,
        mesh=split,
        in_specs=(
            P(None, KV),
            P(KV),
            P(KV, "tp"),
            P(KV, "tp"),
            P(KV, "tp"),
            P(),
            P(None, "tp", KV, None),
            P(None, "tp", KV, None),
            P(None, "tp", KV),
            P(),
            P("tp"),
            P("tp", KV),
            P(KV),
            P(KV, "tp"),
            P("tp", KV),
        ),
        out_specs=P(None, KV),
        check_vma=False,
    )
```
